32 devices in a mesh: ep: 8 (over z, y), tp: 4 (over x, core).
Axes of the slice: x: 2, y: 2, z: 4, core: 2. Of those that a mesh axis runs over, the one named last changes fastest.
Arguments:
- tokens_a: bfloat16 [1024, 2048], P('ep'), may hold values from -30 to 30
- attn_gain: float32 [2048], replicated, may hold values from 0.1 to 1.9
- w_query: bfloat16 [2048, 2048], P(None, 'tp'), may hold values from -2 to 2
- w_query_rot: bfloat16 [2048, 1024], P(None, 'tp'), may hold values from -0.125 to 0.125
- w_latent: bfloat16 [2048, 512], replicated, may hold values from -2 to 2
- w_key_rot: bfloat16 [2048, 32], replicated, may hold values from -0.125 to 0.125
- latent_gain: float32 [512], replicated, may hold values from 0.1 to 1.9
- w_key_up: bfloat16 [512, 2048], P(None, 'tp'), may hold values from -2 to 2
- w_value_up: bfloat16 [512, 2048], P(None, 'tp'), may hold values from -0.25 to 0.25
- w_output: bfloat16 [2048, 2048], P('tp'), may hold values from -0.125 to 0.125
- tokens_b: bfloat16 [2048, 2048], P('ep'), may hold values from -6 to 6
- ffn_gain: float32 [2048], replicated, may hold values from 0.1 to 1.9
- expert_ids: int32 [2048, 2], P('ep'), may hold values from 0 to 7, all different within a row; in each aligned block of 256 rows (0 to 255, 256 to 511, ...) at most 128 rows name the same one
- expert_weights: float32 [2048, 2], P('ep'), may hold values from 0.1 to 1
- w_gate: bfloat16 [8, 2048, 1024], P('ep', None, 'tp'), may hold values from -0.125 to 0.125
- w_up: bfloat16 [8, 2048, 1024], P('ep', None, 'tp'), may hold values from -0.125 to 0.125
- w_down: bfloat16 [8, 1024, 2048], P('ep', 'tp'), may hold values from -0.1875 to 0.1875
Outputs:
- mixed_a: bfloat16 [1024, 2048], P(('ep', 'tp'))
- mixed_b: bfloat16 [2048, 2048], P('ep', 'tp')
The draws below stay inside these ranges and needn't reach their ends.
Inputs may be any that keep to these rules, and one draw needn't show every extreme that they name: `expert_ids`: each row names 2 different experts. In the 256 rows of one index of ep no expert is named more than 128 times, and in some such block one expert is named exactly 128 times.
All inputs are finite; a program needn't handle non-finite values.
Results may differ from the reference program's by a relative error of at most 0.012.
Values may be sent and summed in bfloat16 or wider, within the bound.
A program may use at most 192 MiB of HBM per device.

```python
import math
import jax
import jax.numpy as jnp
import numpy as np
from jax import lax

D = 2048
HEADS = 32
NOPE = 64
ROPE = 32
VD = 64
KVR = 512
FFE = 1024
TOP_K = 2
ROWS_A = 128
ROWS_B = 256
EXPERTS = 8
SEQ_A = 1024
TOKENS_B = 2048
CAP = 128
N_EP = 8
N_TP = 4


def draw_tokens_a(key, part):
    entries = jnp.clip(jax.random.normal(jax.random.fold_in(key, 11), (SEQ_A, D), jnp.float32), -6.0, 6.0)
    return entries.astype(jnp.bfloat16)


def draw_w_query(key, part):
    drawn = jnp.clip(jax.random.normal(jax.random.fold_in(key, 21), (D, HEADS * NOPE), jnp.float32), -6.0, 6.0)
    drawn = drawn * D ** (-0.5)
    return jnp.clip(drawn, -2.0, 2.0).astype(jnp.bfloat16)


def draw_w_latent(key, part):
    drawn = jnp.clip(jax.random.normal(jax.random.fold_in(key, 31), (D, KVR), jnp.float32), -6.0, 6.0)
    drawn = drawn * D ** (-0.5)
    return jnp.clip(drawn, -2.0, 2.0).astype(jnp.bfloat16)


def draw_w_key_up(key, part):
    drawn = jnp.clip(jax.random.normal(jax.random.fold_in(key, 41), (KVR, HEADS * NOPE), jnp.float32), -6.0, 6.0)
    drawn = drawn * KVR ** (-0.5)
    return jnp.clip(drawn, -2.0, 2.0).astype(jnp.bfloat16)


def block_levels(own_key, extent, cuts, low, high):
    level = 1.0
    for dim, parts in cuts:
        draws = jax.random.uniform(jax.random.fold_in(jax.random.fold_in(own_key, 6), dim), (parts,), jnp.float32, low / len(cuts), high / len(cuts))
        level = level * jnp.repeat(jnp.exp(draws), extent[dim] // parts).reshape((-1,) + (1,) * (len(extent) - 1 - dim))
    return level


def deal_out(rng, own, number, rows, amount, top, limit, skew):
    sequence = jax.random.permutation(rng, amount)
    heavy_load, usual = portions_of(amount, rows * top, limit, skew, True), portions_of(amount, rows * top, limit, skew, False)
    places = jnp.arange(amount)

    def named(tallies, turn):
        used = int((tallies > 0).sum())
        fixed = max(1, used // 4)
        moved = fixed + (places - fixed + turn * (used - fixed)) % max(1, amount - fixed)
        return jnp.zeros((amount,), jnp.int32).at[sequence[jnp.where(places < fixed, places, moved)]].set(jnp.asarray(tallies, jnp.int32))

    tallies = jnp.where(number % 4 == 0, named(heavy_load, number // 4), named(usual, number - number // 4 - 1))
    mixed = jax.random.permutation(jax.random.fold_in(own, 3), amount)
    giver, taker = mixed[0:amount // 2 * 2:2], mixed[1:amount // 2 * 2:2]
    room = jnp.minimum(tallies[giver] - 1, limit - tallies[taker]) // 2
    room = jnp.where((giver == sequence[0]) | (taker == sequence[0]) | (tallies[taker] == 0), 0, jnp.maximum(room, 0))
    moved = jax.random.randint(jax.random.fold_in(own, 4), (amount // 2,), 0, 1 << 20) % (room + 1)
    tallies = tallies.at[giver].add(-moved).at[taker].add(moved)
    labels = jnp.searchsorted(jnp.cumsum(tallies), jnp.arange(rows * top), side="right").astype(jnp.int32)
    grid = labels.reshape(top, rows).T
    grid = grid[jax.random.permutation(jax.random.fold_in(own, 1), rows)]
    turn = jax.random.randint(jax.random.fold_in(own, 2), (rows, 1), 0, top)
    return jnp.take_along_axis(grid, (jnp.arange(top)[None, :] + turn) % top, axis=1)


def portions_of(amount, total, most, lean, full):
    weights = [(1 << 20) // math.isqrt(grade ** lean) + 1 for grade in range(1, amount + 1)]
    largest = most if full else min(most, max(-(-total // amount), total * weights[0] // sum(weights)))
    least = 1 if total - largest >= amount - 1 else 0
    given, surplus = [largest] + [least] * (amount - 1), total - largest - least * (amount - 1)
    while surplus > 0:
        movable = [i for i in range(1, amount) if given[i] < largest] or [i for i in range(1, amount) if given[i] < most]
        pool, left = sum([weights[i] for i in movable]), surplus
        for i in movable:
            more = min(most - given[i], max(1, left * weights[i] // pool), surplus)
            given[i] = given[i] + more
            surplus = surplus - more
    return np.array(given)


def scatter_about(key, dims, scale, reach, cuts=(), kind=jnp.bfloat16):
    level = block_levels(key, dims, cuts, -0.22, 0.18) if cuts else 1.0
    values = jax.random.normal(key, dims, jnp.float32) * scale * level
    return jnp.minimum(jnp.maximum(values, -reach), reach).astype(kind)


def setup_inputs(seed: int = 0) -> dict:
    seeds = jax.random.split(jax.random.key(seed), 18)
    tokens_a = draw_tokens_a(jax.random.fold_in(seeds[17], 71), 0)
    attn_gain = jnp.clip(1.0 + 0.18 * jax.random.normal(seeds[1], (D,), jnp.float32), 0.1, 1.9)
    w_query = draw_w_query(jax.random.fold_in(seeds[17], 71), 0)
    w_query_rot = scatter_about(seeds[3], (D, HEADS * ROPE), D ** -0.5, 0.125, ((1, 4),))
    w_latent = draw_w_latent(jax.random.fold_in(seeds[17], 71), 0)
    w_key_rot = scatter_about(seeds[5], (D, ROPE), D ** -0.5, 0.125)
    latent_gain = jnp.clip(1.0 + 0.18 * jax.random.normal(seeds[6], (KVR,), jnp.float32), 0.1, 1.9)
    w_key_up = draw_w_key_up(jax.random.fold_in(seeds[17], 71), 0)
    w_value_up = scatter_about(seeds[8], (KVR, HEADS * VD), KVR ** -0.5, 0.25, ((1, 4),))
    w_output = scatter_about(seeds[9], (HEADS * VD, D), (HEADS * VD) ** -0.5, 0.125, ((0, 4),))
    tokens_b = scatter_about(seeds[10], (TOKENS_B, D), 1.0, 6.0, ((0, 8),))
    ffn_gain = jnp.clip(1.0 + 0.18 * jax.random.normal(seeds[11], (D,), jnp.float32), 0.1, 1.9)
    expert_ids_keys = jax.random.split(jax.random.fold_in(seeds[12], 1), TOKENS_B // ROWS_B)
    expert_ids_turns = jax.random.permutation(jax.random.fold_in(seeds[12], 3), TOKENS_B // ROWS_B)
    expert_ids = jax.vmap(lambda own, number: deal_out(jax.random.fold_in(seeds[12], 2), own, number, ROWS_B, EXPERTS, TOP_K, CAP, 1))(expert_ids_keys, expert_ids_turns).reshape((TOKENS_B, TOP_K))
    expert_weights = jnp.clip(0.1 + 0.9 * jax.random.uniform(seeds[13], (TOKENS_B, TOP_K), jnp.float32) ** block_levels(seeds[13], (TOKENS_B, TOP_K), ((0, 8),), -0.2, 0.2), 0.1, 1.0)
    w_gate = scatter_about(seeds[14], (EXPERTS, D, FFE), D ** -0.5, 0.125, ((0, 8), (2, 4)))
    w_up = scatter_about(seeds[15], (EXPERTS, D, FFE), D ** -0.5, 0.125, ((0, 8), (2, 4)))
    w_down = scatter_about(seeds[16], (EXPERTS, FFE, D), FFE ** -0.5, 0.1875, ((0, 8), (1, 4)))
    return dict(tokens_a=tokens_a, attn_gain=attn_gain, w_query=w_query, w_query_rot=w_query_rot, w_latent=w_latent, w_key_rot=w_key_rot, latent_gain=latent_gain, w_key_up=w_key_up, w_value_up=w_value_up, w_output=w_output, tokens_b=tokens_b, ffn_gain=ffn_gain, expert_ids=expert_ids, expert_weights=expert_weights, w_gate=w_gate, w_up=w_up, w_down=w_down)


epsilon = 1e-06
rope_base = 10000.0

def normalize(matrix, gain):
    floats = matrix.astype(jnp.float32)
    scaled = floats * lax.rsqrt(lax.optimization_barrier(jnp.mean(floats * floats, axis=-1, keepdims=True)) + epsilon)
    return scaled * gain.astype(jnp.float32)

def rotate(vectors, positions):
    rot_width = vectors.shape[-1]
    half_width = rot_width // 2
    inverse = rope_base ** (-(jnp.arange(half_width, dtype=jnp.float32) * 2.0) / rot_width)
    angles = positions.astype(jnp.float32)[:, None] * inverse[None, :]
    cosine = jnp.cos(angles)[:, None, :]
    sine_part = jnp.sin(angles)[:, None, :]
    first_half = vectors[..., :half_width]
    second_half = vectors[..., half_width:]
    return jnp.concatenate([first_half * cosine - second_half * sine_part, first_half * sine_part + second_half * cosine], axis=-1)

def attention_half(tokens_a, attn_gain, w_query, w_query_rot, w_latent, w_key_rot, latent_gain, w_key_up, w_value_up, w_output):
    positions = jnp.arange(SEQ_A, dtype=jnp.int32)
    normed = normalize(tokens_a, attn_gain).astype(jnp.bfloat16)
    query_plain = jnp.dot(normed, w_query, preferred_element_type=jnp.float32).astype(jnp.bfloat16)
    query_plain = query_plain.reshape(N_EP, ROWS_A, HEADS, NOPE)
    turned = jnp.dot(normed, w_query_rot, preferred_element_type=jnp.float32).reshape(SEQ_A, HEADS, ROPE)
    query_rotated_rows = rotate(turned, positions).astype(jnp.bfloat16).reshape(N_EP, ROWS_A, HEADS, ROPE)
    latent = normalize(jnp.dot(normed, w_latent, preferred_element_type=jnp.float32), latent_gain).astype(jnp.bfloat16)
    key_raw = jnp.dot(normed, w_key_rot, preferred_element_type=jnp.float32)[:, None, :]
    key_turned = rotate(key_raw, positions)[:, 0, :].astype(jnp.bfloat16)
    key_plain = jnp.dot(latent, w_key_up, preferred_element_type=jnp.float32).astype(jnp.bfloat16)
    values = jnp.dot(latent, w_value_up, preferred_element_type=jnp.float32).astype(jnp.bfloat16)
    key_wide_float = key_plain.astype(jnp.float32).reshape(N_EP, ROWS_A, HEADS, NOPE)
    rotated_key_float = key_turned.astype(jnp.float32).reshape(N_EP, ROWS_A, ROPE)
    value_float = values.astype(jnp.float32).reshape(N_EP, ROWS_A, HEADS, VD)
    key_pos = positions.reshape(N_EP, ROWS_A)
    logit_scale = (NOPE + ROPE) ** (-0.5)

    def one_block(inputs):
        query_tile_block, rotated_key_block, query_pos = inputs
        score_matrix = (jnp.einsum('yvz,wrvz->yvwr', query_tile_block.astype(jnp.float32), key_wide_float) + jnp.einsum('yjx,inx->yjin', rotated_key_block.astype(jnp.float32), rotated_key_float)) * logit_scale
        allowed = key_pos[None, None, :, :] <= query_pos[:, None, None, None]
        masked = jnp.where(allowed, score_matrix, -1e+30)
        block_max = lax.optimization_barrier(jnp.max(masked, axis=-1))
        probs = jnp.where(allowed, jnp.exp(masked - block_max[..., None]), 0.0)
        block_total = lax.optimization_barrier(jnp.sum(probs, axis=-1))
        rounded = probs.astype(jnp.bfloat16).astype(jnp.float32)
        block_out = jnp.einsum('qhbk,bkhd->qhbd', rounded, value_float)
        overall = lax.optimization_barrier(jnp.max(block_max, axis=-1))
        factor = jnp.exp(block_max - overall[..., None])
        denominator = lax.optimization_barrier(jnp.sum(factor * block_total, axis=-1))
        merged = lax.optimization_barrier(jnp.sum(factor[..., None] * block_out, axis=2))
        return (merged / denominator[..., None]).astype(jnp.bfloat16).reshape(ROWS_A, HEADS * VD)
    attended = lax.map(one_block, (query_plain, query_rotated_rows, key_pos)).reshape(SEQ_A, HEADS * VD)
    group_width = HEADS // N_TP * VD
    summed = jnp.zeros((SEQ_A, D), jnp.float32)
    for lane_index in range(N_TP):
        lane_part = jnp.dot(attended[:, lane_index * group_width:(lane_index + 1) * group_width], w_output[lane_index * group_width:(lane_index + 1) * group_width], preferred_element_type=jnp.float32)
        summed = summed + lax.optimization_barrier(lane_part.astype(jnp.bfloat16)).astype(jnp.float32)
    return summed.astype(jnp.bfloat16)

def expert_half(tokens_b, ffn_gain, expert_ids, expert_weights, w_gate, w_up, w_down):
    normed = normalize(tokens_b, ffn_gain).astype(jnp.bfloat16)
    block_pairs = ROWS_B * TOP_K
    flat_ids = expert_ids.reshape(N_EP, block_pairs)
    onehot = (flat_ids[:, :, None] == jnp.arange(EXPERTS, dtype=jnp.int32)[None, None, :]).astype(jnp.int32)
    before = jnp.cumsum(onehot, axis=1) - onehot
    slot_index = lax.optimization_barrier(jnp.sum(before * onehot, axis=2))
    block_index = jnp.arange(N_EP, dtype=jnp.int32)[:, None]
    target = (flat_ids * (N_EP * CAP) + block_index * CAP + slot_index).reshape(-1).astype(jnp.int32)
    total_slots = EXPERTS * N_EP * CAP
    pair_total = TOKENS_B * TOP_K
    source_row = jnp.zeros((total_slots,), jnp.int32).at[target].set(jnp.arange(pair_total, dtype=jnp.int32) // TOP_K)
    occupied = jnp.zeros((total_slots,), jnp.int32).at[target].set(1)
    table = source_row.reshape(EXPERTS, N_EP * CAP)
    filled = occupied.reshape(EXPERTS, N_EP * CAP)
    lane_width = FFE // N_TP

    def one_expert(inputs):
        rows_of, filled_of, gate_weight, up_weight, down_weight = inputs
        taken_rows = jnp.where(filled_of[:, None] > 0, normed[rows_of], jnp.zeros((), jnp.bfloat16))
        gate_part = jnp.dot(taken_rows, gate_weight, preferred_element_type=jnp.float32)
        up_part = jnp.dot(taken_rows, up_weight, preferred_element_type=jnp.float32)
        hidden = (jax.nn.silu(gate_part) * up_part).astype(jnp.bfloat16)
        summed = jnp.zeros((taken_rows.shape[0], D), jnp.float32)
        for lane_index in range(N_TP):
            lane_part = jnp.dot(hidden[:, lane_index * lane_width:(lane_index + 1) * lane_width], down_weight[lane_index * lane_width:(lane_index + 1) * lane_width], preferred_element_type=jnp.float32)
            summed = summed + lax.optimization_barrier(lane_part.astype(jnp.bfloat16)).astype(jnp.float32)
        return summed.astype(jnp.bfloat16)
    outputs = lax.map(one_expert, (table, filled, w_gate, w_up, w_down))
    picked = outputs.reshape(total_slots, D)[target].astype(jnp.float32).reshape(TOKENS_B, TOP_K, D)
    shares = expert_weights / lax.optimization_barrier(jnp.sum(expert_weights, axis=1, keepdims=True))
    return lax.optimization_barrier(jnp.sum(picked * shares[:, :, None], axis=1)).astype(jnp.bfloat16)

def reference(tokens_a, attn_gain, w_query, w_query_rot, w_latent, w_key_rot, latent_gain, w_key_up, w_value_up, w_output, tokens_b, ffn_gain, expert_ids, expert_weights, w_gate, w_up, w_down):
    mixed_a = attention_half(tokens_a, attn_gain, w_query, w_query_rot, w_latent, w_key_rot, latent_gain, w_key_up, w_value_up, w_output)
    mixed_b = expert_half(tokens_b, ffn_gain, expert_ids, expert_weights, w_gate, w_up, w_down)
    return (mixed_a, mixed_b)
```

```python
import dataclasses
import functools
import math

import jax
import jax.numpy as jnp
import numpy as np
from jax import lax
from jax.experimental import pallas as pl
from jax.experimental.pallas import tpu as pltpu
from jax.sharding import PartitionSpec as P

NOPE = 64
ROPE = 32
VD = 64
LANES = 128
VMEM_BYTES = 60 * 1024 * 1024


epsilon = 1e-06
rope_base = 10000.0


def normalize(matrix, gain):
    floats = matrix.astype(jnp.float32)
    scaled = floats * lax.rsqrt(jnp.mean(floats * floats, axis=-1, keepdims=True) + epsilon)
    return scaled * gain


def rotate(vectors, positions):
    rot_width = vectors.shape[-1]
    half_width = rot_width // 2
    inverse = rope_base ** (-(jnp.arange(half_width, dtype=jnp.float32) * 2.0) / rot_width)
    angles = positions.astype(jnp.float32)[:, None] * inverse[None, :]
    cosine = jnp.cos(angles)[:, None, :]
    sine_part = jnp.sin(angles)[:, None, :]
    first_half = vectors[..., :half_width]
    second_half = vectors[..., half_width:]
    return jnp.concatenate(
        [
            first_half * cosine - second_half * sine_part,
            first_half * sine_part + second_half * cosine,
        ],
        axis=-1,
    )


def attention_half(
    tokens_a,
    attn_gain,
    w_query,
    w_query_rot,
    w_latent,
    w_key_rot,
    latent_gain,
    w_key_up,
    w_value_up,
    w_output,
    outgoing,
):
    row_count = tokens_a.shape[0]
    head_count = w_query.shape[1] // NOPE
    offset = lax.axis_index("ep") * row_count
    positions = offset + jnp.arange(row_count, dtype=jnp.int32)
    normed = normalize(tokens_a, attn_gain).astype(jnp.bfloat16)
    query_plain = jnp.dot(normed, w_query, preferred_element_type=jnp.float32).astype(jnp.bfloat16)
    query_plain = query_plain.reshape(row_count, head_count, NOPE)
    turned = jnp.dot(normed, w_query_rot, preferred_element_type=jnp.float32).reshape(
        row_count, head_count, ROPE
    )
    query_rotated_rows = rotate(turned, positions).astype(jnp.bfloat16)
    latent = normalize(
        jnp.dot(normed, w_latent, preferred_element_type=jnp.float32), latent_gain
    ).astype(jnp.bfloat16)
    key_raw = jnp.dot(normed, w_key_rot, preferred_element_type=jnp.float32)[:, None, :]
    key_turned = rotate(key_raw, positions)[:, 0, :].astype(jnp.bfloat16)
    logit_scale = (NOPE + ROPE) ** (-0.5)
    outgoing, compact = lax.optimization_barrier(
        (outgoing, jnp.concatenate([latent, key_turned], axis=1))
    )
    joined = lax.all_gather(compact, "ep", axis=0, tiled=True)
    arrived = lax.all_to_all(outgoing, "ep", split_axis=0, concat_axis=0, tiled=True)
    pieces = (joined[:, : latent.shape[1]], joined[:, latent.shape[1] :])
    piece_keys = jnp.dot(pieces[0], w_key_up, preferred_element_type=jnp.float32).astype(
        jnp.bfloat16
    )
    piece_values = jnp.dot(pieces[0], w_value_up, preferred_element_type=jnp.float32).astype(
        jnp.bfloat16
    )
    key_count = piece_keys.shape[0]
    blocks = key_count // row_count
    key_blocks = piece_keys.reshape(blocks, row_count, head_count, NOPE)
    value_blocks = piece_values.reshape(blocks, row_count, head_count, VD)
    rotated_key_blocks = pieces[1].reshape(blocks, row_count, ROPE)
    score_matrix = (
        jnp.einsum("yvz,wrvz->yvwr", query_plain, key_blocks, preferred_element_type=jnp.float32)
        + jnp.einsum(
            "yjx,inx->yjin",
            query_rotated_rows,
            rotated_key_blocks,
            preferred_element_type=jnp.float32,
        )
    ) * logit_scale
    key_pos = jnp.arange(key_count, dtype=jnp.int32).reshape(blocks, row_count)
    allowed = key_pos[None, None, :, :] <= positions[:, None, None, None]
    masked = jnp.where(allowed, score_matrix, -1e30)
    block_max = jnp.max(masked, axis=-1)
    probs = jnp.where(allowed, jnp.exp(masked - block_max[..., None]), 0.0)
    block_total = jnp.sum(probs, axis=-1)
    block_out = jnp.einsum(
        "qhbk,bkhd->qhbd",
        probs.astype(jnp.bfloat16),
        value_blocks,
        preferred_element_type=jnp.float32,
    )
    run_max = jnp.full((row_count, head_count), -1e30, jnp.float32)
    new_max = jnp.maximum(run_max, jnp.max(block_max, axis=-1))
    new_factor = jnp.exp(block_max - new_max[..., None])
    new_total = jnp.sum(new_factor * block_total, axis=-1)
    new_out = jnp.sum(new_factor[..., None] * block_out, axis=2)
    attended = (
        (new_out / new_total[..., None]).astype(jnp.bfloat16).reshape(row_count, head_count * VD)
    )
    mixed = lax.psum_scatter(
        jnp.dot(attended, w_output, preferred_element_type=jnp.float32).astype(jnp.bfloat16),
        "tp",
        scatter_dimension=0,
        tiled=True,
    )
    return mixed, arrived


def dispatch_rows(tokens_b, ffn_gain, expert_ids, expert_count):
    row_count, width = tokens_b.shape
    top_count = expert_ids.shape[1]
    capacity = 2 * row_count * top_count // expert_count
    tp_count = lax.axis_size("tp")
    part_width = width // tp_count
    floats = tokens_b.astype(jnp.float32)
    factor = lax.rsqrt(jnp.mean(floats * floats, axis=-1, keepdims=True) + epsilon)
    start = lax.axis_index("tp") * part_width
    own = lax.dynamic_slice_in_dim(tokens_b, start, part_width, 1).astype(jnp.float32)
    own_gain = lax.dynamic_slice_in_dim(ffn_gain, start, part_width, 0)
    normed = (own * factor * own_gain).astype(jnp.bfloat16)
    experts = jnp.arange(expert_count, dtype=jnp.int32)
    slots = jnp.arange(capacity, dtype=jnp.int32)
    named = (expert_ids[:, :, None] == experts).any(axis=1)
    rows = jnp.arange(row_count, dtype=jnp.int32)
    earlier = (rows[:, None] > rows[None, :]).astype(jnp.bfloat16)
    before = jnp.dot(
        earlier, named.astype(jnp.bfloat16), preferred_element_type=jnp.float32
    ).astype(jnp.int32)
    slot_of = jnp.where(named, before, -1).T
    chosen = (slot_of[:, None, :] == slots[None, :, None]).astype(jnp.bfloat16)
    outgoing = jnp.dot(
        chosen.reshape(expert_count * capacity, row_count),
        normed,
        preferred_element_type=jnp.float32,
    ).astype(jnp.bfloat16)
    outgoing = outgoing.reshape(expert_count, capacity, part_width)
    return outgoing, before


def swap(block, distance, count):
    return lax.ppermute(block, "tp", [(i, i ^ distance) for i in range(count)])


def expert_half(arrived, before, expert_ids, expert_weights, w_gate, w_up, w_down):
    expert_count, capacity, part_width = arrived.shape
    tp_count = lax.axis_size("tp")
    top_count = expert_ids.shape[1]
    experts = jnp.arange(expert_count, dtype=jnp.int32)
    me = lax.axis_index("tp")
    blocks = {0: arrived.reshape(-1, part_width)}
    distance = tp_count // 2
    while distance:
        for mask in list(blocks):
            blocks[mask ^ distance] = swap(blocks[mask], distance, tp_count)
        distance //= 2
    gate_part = 0.0
    up_part = 0.0
    for mask, block in blocks.items():
        first = (me ^ mask) * part_width
        gate_rows = lax.dynamic_slice_in_dim(w_gate[0], first, part_width, 0)
        up_rows = lax.dynamic_slice_in_dim(w_up[0], first, part_width, 0)
        gate_part += jnp.dot(block, gate_rows, preferred_element_type=jnp.float32)
        up_part += jnp.dot(block, up_rows, preferred_element_type=jnp.float32)
    hidden = (jax.nn.silu(gate_part) * up_part).astype(jnp.bfloat16)
    parts = {}
    for mask in reversed(range(tp_count)):
        down_columns = lax.dynamic_slice_in_dim(w_down[0], (me ^ mask) * part_width, part_width, 1)
        parts[mask] = jnp.dot(hidden, down_columns, preferred_element_type=jnp.float32)
    distance = 1
    while distance < tp_count:
        for mask in [m for m in parts if m & distance]:
            came = swap(parts.pop(mask).astype(jnp.bfloat16), distance, tp_count)
            parts[mask ^ distance] += came.astype(jnp.float32)
        distance *= 2
    summed = parts[0].astype(jnp.bfloat16)
    returned = lax.all_to_all(
        summed.reshape(expert_count, capacity, part_width),
        "ep",
        split_axis=0,
        concat_axis=0,
        tiled=True,
    )
    shares = expert_weights / jnp.sum(expert_weights, axis=1, keepdims=True)
    table = returned.reshape(expert_count * capacity, part_width)
    total = 0.0
    for k in range(top_count):
        own_slot = jnp.sum(jnp.where(expert_ids[:, k : k + 1] == experts, before, 0), axis=1)
        target = expert_ids[:, k] * capacity + own_slot
        pick = (
            target[:, None] == jnp.arange(expert_count * capacity, dtype=jnp.int32)
        ).astype(jnp.bfloat16)
        picked = jnp.dot(pick, table, preferred_element_type=jnp.float32)
        total = total + picked * shares[:, k : k + 1]
    return total.astype(jnp.bfloat16)


def rope_tables(rows, blocks):
    half = ROPE // 2
    lane = np.arange(LANES) % ROPE
    inverse = rope_base ** (-((lane % half).astype(np.float64) * 2.0) / ROPE)
    near = np.arange(rows, dtype=np.float64)[:, None] * inverse[None, :]
    far = (np.arange(blocks, dtype=np.float64) * rows)[:, None] * inverse[None, :]
    pack = lambda v: np.asarray(v, np.float32)
    return pack(np.stack([np.cos(near), np.sin(near)])), pack(
        np.stack([np.cos(far), np.sin(far)], axis=1)
    )


def fused_kernel(
    dims,
    ta_hbm, ag_ref, wq_hbm, wqr_hbm, wl_hbm, wkr_hbm, lg_ref, wku_hbm, wvu_hbm, wo_hbm,
    tb_hbm, fg_ref, ids_ref, wts_ref, wg_hbm, wu_hbm, wd_hbm, near_ref, far_ref,
    out_a, out_b,
    ta, wq, wqr, wl, wkr, wku, wvu, wo, tb, wg, wu, wd,
    own_b, slot_t, slot_c, share_c, staged, landed, part_keep, part_send, part_recv,
    pair_send, pair_recv, back_send, back_recv, total,
    normed_a, rot_w, lat, qs, keys, vals, att, mixed, am_send, am_recv, ax_send, ax_recv,
    load_sem, z_send, z_recv, x_send, x_recv, c_send, c_recv, f_send, f_recv,
    p_send, p_recv, q_send, q_recv, b_send, b_recv,
    lz_send, lz_recv, ly_send, ly_recv, ld_send, ld_recv, as_send, as_recv, at_send, at_recv,
):
    n, cap, rows_a, rows_b = dims.n, dims.cap, dims.rows_a, dims.rows_b
    width = dims.width
    e, t = lax.axis_index("ep"), lax.axis_index("tp")
    core = lax.rem(t, 2)
    mate, across = t + 1 - 2 * core, lax.rem(t + 2, 4)
    third = lax.rem(mate + 2, 4)
    quarter = (t, mate, across, third)
    beside = e + 1 - 2 * lax.rem(e, 2)

    def plus(k):
        return lax.rem(e + k, n)

    def minus(k):
        return lax.rem(e + n - k, n)

    def remote(src, dst, ssem, rsem, ep=None, tp=None):
        target = (e if ep is None else ep, t if tp is None else tp)
        return pltpu.make_async_remote_copy(
            src_ref=src, dst_ref=dst, send_sem=ssem, recv_sem=rsem,
            device_id=target, device_id_type=pl.DeviceIdType.MESH,
        )

    pairs = [
        (tb_hbm, tb), (ta_hbm, ta), (wl_hbm, wl), (wkr_hbm, wkr), (wg_hbm, wg), (wu_hbm, wu),
        (wd_hbm, wd), (wq_hbm, wq), (wqr_hbm, wqr), (wku_hbm, wku), (wvu_hbm, wvu), (wo_hbm, wo),
    ]
    loads = [pltpu.make_async_copy(s, d, load_sem.at[i]) for i, (s, d) in enumerate(pairs)]
    for load in loads:
        load.start()
    (l_tb, l_ta, l_wl, l_wkr, l_wg, l_wu, l_wd, l_wq, l_wqr, l_wku, l_wvu, l_wo) = loads

    barrier = pltpu.get_barrier_semaphore()
    for k in range(1, n):
        pl.semaphore_signal(
            barrier, inc=1, device_id=(plus(k), t), device_id_type=pl.DeviceIdType.MESH
        )
    for peer in (mate, across):
        pl.semaphore_signal(
            barrier, inc=1, device_id=(e, peer), device_id_type=pl.DeviceIdType.MESH
        )

    def own_columns(which):
        return pl.ds(pl.multiple_of(which * width, width), width)

    ids = ids_ref[...]
    sub = lax.broadcasted_iota(jnp.int32, (LANES, rows_b), 0)
    first, second = ids[0:1] == sub, ids[1:2] == sub
    named = jnp.logical_or(first, second)
    earlier = (
        lax.broadcasted_iota(jnp.int32, (rows_b, rows_b), 0)
        < lax.broadcasted_iota(jnp.int32, (rows_b, rows_b), 1)
    ).astype(jnp.float32).astype(jnp.bfloat16)
    before = jnp.dot(
        named.astype(jnp.float32).astype(jnp.bfloat16), earlier, preferred_element_type=jnp.float32
    )
    slot = jnp.where(named, before, -1.0)
    slot_t[...] = slot
    slot_c[...] = slot.T
    weight = wts_ref[...]
    sum_weight = weight[0:1] + weight[1:2]
    share_c[...] = (
        jnp.where(first, weight[0:1] / sum_weight, 0.0)
        + jnp.where(second, weight[1:2] / sum_weight, 0.0)
    ).T

    l_tb.wait()
    floats = tb[...].astype(jnp.float32)
    factor = lax.rsqrt(jnp.mean(floats * floats, axis=-1, keepdims=True) + epsilon)
    columns = own_columns(t)
    own_b[...] = (
        tb[:, columns].astype(jnp.float32) * factor * fg_ref[:, columns]
    ).astype(jnp.bfloat16)

    pl.semaphore_wait(barrier, n + 1)

    def z_copy(m):
        return remote(staged.at[m], landed.at[0, m], z_send.at[m], z_recv.at[m], ep=plus(m))

    def x_copy(m):
        return remote(landed.at[0, m], landed.at[2, m], x_send.at[m], x_recv.at[m], tp=across)

    def c_copy(m):
        return remote(landed.at[0, m], landed.at[1, m], c_send.at[m], c_recv.at[m], tp=mate)

    def f_copy(m):
        return remote(landed.at[2, m], landed.at[3, m], f_send.at[m], f_recv.at[m], tp=mate)

    def p_copy(m):
        return remote(part_send.at[m], part_recv.at[m], p_send.at[m], p_recv.at[m], tp=mate)

    def q_copy(m):
        return remote(pair_send.at[m], pair_recv.at[m], q_send.at[m], q_recv.at[m], tp=across)

    def b_copy(m):
        return remote(back_send.at[m], back_recv.at[m], b_send.at[m], b_recv.at[m], ep=minus(m))

    def dispatch(m):
        row = slot_t[pl.ds(plus(m), 1), :]
        wanted = lax.broadcasted_iota(jnp.int32, (cap, rows_b), 0).astype(jnp.float32)
        chosen = (row == wanted).astype(jnp.float32).astype(jnp.bfloat16)
        picked = jnp.dot(chosen, own_b[...], preferred_element_type=jnp.float32)
        if m:
            staged[m] = picked.astype(jnp.bfloat16)
            z_copy(m).start()
        else:
            landed[0, 0] = picked.astype(jnp.bfloat16)
            x_copy(0).start()
            c_copy(0).start()

    def forward(m):
        z_copy(m).wait_recv()
        x_copy(m).start()
        c_copy(m).start()

    def relay(m):
        x_copy(m).wait_recv()
        f_copy(m).start()

    def expert(m):
        c_copy(m).wait_recv()
        f_copy(m).wait_recv()
        gate = up = None
        for mask in range(4):
            at = own_columns(quarter[mask])
            block = landed[mask, m]
            g = jnp.dot(block, wg[0, at, :], preferred_element_type=jnp.float32)
            u = jnp.dot(block, wu[0, at, :], preferred_element_type=jnp.float32)
            gate, up = (g, u) if mask == 0 else (gate + g, up + u)
        hidden = (gate / (1.0 + jnp.exp(-gate)) * up).astype(jnp.bfloat16)
        for place, mask in enumerate((1, 3)):
            part_send[m, place] = jnp.dot(
                hidden, wd[0, :, own_columns(quarter[mask])], preferred_element_type=jnp.float32
            ).astype(jnp.bfloat16)
        p_copy(m).start()
        for place, mask in enumerate((0, 2)):
            part_keep[m, place] = jnp.dot(
                hidden, wd[0, :, own_columns(quarter[mask])], preferred_element_type=jnp.float32
            )

    def pair_sum(m):
        p_copy(m).wait_recv()
        pair_send[m] = (part_keep[m, 1] + part_recv[m, 1].astype(jnp.float32)).astype(jnp.bfloat16)
        q_copy(m).start()
        part_keep[m, 0] = part_keep[m, 0] + part_recv[m, 0].astype(jnp.float32)

    def give_back(m):
        q_copy(m).wait_recv()
        summed = (part_keep[m, 0] + pair_recv[m].astype(jnp.float32)).astype(jnp.bfloat16)
        if m:
            back_send[m] = summed
            b_copy(m).start()
        else:
            back_recv[0] = summed

    def combine(m, begin=False):
        if m:
            b_copy(m).wait_recv()
        expert_at = plus(m)
        lane = lax.broadcasted_iota(jnp.int32, (rows_b, LANES), 1)
        here = lane == expert_at
        at = jnp.sum(jnp.where(here, slot_c[...], 0.0), axis=1, keepdims=True)
        share = jnp.sum(jnp.where(here, share_c[...], 0.0), axis=1, keepdims=True)
        wanted = lax.broadcasted_iota(jnp.int32, (rows_b, cap), 1).astype(jnp.float32)
        pick = (at == wanted).astype(jnp.float32).astype(jnp.bfloat16)
        picked = jnp.dot(pick, back_recv[m], preferred_element_type=jnp.float32) * share
        total[...] = picked if begin else total[...] + picked

    half_rows = rows_a // 2
    mine = pl.ds(pl.multiple_of(core * half_rows, half_rows), half_rows)
    quads = n // 2

    def lz_copy(k):
        return remote(
            lat.at[e, mine], lat.at[e, mine], lz_send.at[k], lz_recv.at[k], ep=plus(2 * k)
        )

    def lz_arrival(k):
        block = lat.at[minus(2 * k), mine]
        return remote(block, block, lz_send.at[k], lz_recv.at[k], ep=plus(2 * k))

    def ly_copy(k):
        block = lat.at[minus(2 * k), mine]
        return remote(block, block, ly_send.at[k], ly_recv.at[k], ep=beside)

    def ly_arrival(k):
        block = lat.at[lax.rem(beside + n - 2 * k, n), mine]
        return remote(block, block, ly_send.at[k], ly_recv.at[k], ep=beside)

    yours = pl.ds(pl.multiple_of((1 - core) * half_rows, half_rows), half_rows)

    def ld_copy(j, owner, part=None):
        block = lat.at[owner, mine if part is None else part]
        return remote(block, block, ld_send.at[j], ld_recv.at[j], tp=mate)

    def owner_of(j):
        return minus(2 * j) if j < quads else lax.rem(beside + n - 2 * (j - quads), n)

    def latents():
        l_ta.wait()
        rows = ta[...].astype(jnp.float32)
        scale = lax.rsqrt(jnp.mean(rows * rows, axis=-1, keepdims=True) + epsilon)
        normed_a[...] = (rows * scale * ag_ref[...]).astype(jnp.bfloat16)
        l_wl.wait()
        raw = jnp.dot(normed_a[...], wl[...], preferred_element_type=jnp.float32)
        scale = lax.rsqrt(jnp.mean(raw * raw, axis=-1, keepdims=True) + epsilon)
        lat[e, :, : dims.rank] = (raw * scale * lg_ref[...]).astype(jnp.bfloat16)
        l_wkr.wait()
        plain = wkr[...]
        swapped = jnp.concatenate([-plain[ROPE // 2 :], plain[: ROPE // 2]], axis=0)
        for copy in range(LANES // ROPE):
            rot_w[copy * ROPE : (copy + 1) * ROPE] = plain
            rot_w[LANES + copy * ROPE : LANES + (copy + 1) * ROPE] = swapped
        both = lax.dot_general(
            normed_a[...], rot_w[...], (((1,), (1,)), ((), ())), preferred_element_type=jnp.float32
        )
        cosine, sine = turn()
        lat[e, :, dims.rank :] = (both[:, :LANES] * cosine + both[:, LANES:] * sine).astype(
            jnp.bfloat16
        )
        for k in range(1, quads):
            lz_copy(k).start()
        ly_copy(0).start()

    def turn():
        far = far_ref[e]
        cosine = near_ref[0] * far[0:1] - near_ref[1] * far[1:2]
        sine = near_ref[1] * far[0:1] + near_ref[0] * far[1:2]
        return cosine, sine

    def latents_on():
        for k in range(1, quads):
            lz_arrival(k).wait_recv()
            ly_copy(k).start()
            ld_copy(k, owner_of(k)).start()

    def latents_over():
        for k in range(quads):
            ly_arrival(k).wait_recv()
            ld_copy(quads + k, owner_of(quads + k)).start()

    def latents_in():
        for j in range(1, n):
            ld_copy(j, owner_of(j), yours).wait_recv()

    def queries():
        l_wq.wait()
        l_wqr.wait()
        plain = jnp.dot(normed_a[...], wq[...], preferred_element_type=jnp.float32).astype(
            jnp.bfloat16
        )
        raw = jnp.dot(normed_a[...], wqr[...], preferred_element_type=jnp.float32)
        cosine, sine = turn()
        lane = lax.broadcasted_iota(jnp.int32, (rows_a, LANES), 1)
        low = lax.rem(lane, ROPE) < ROPE // 2
        turned = []
        for g in range(raw.shape[1] // LANES):
            x = raw[:, g * LANES : (g + 1) * LANES]
            other = jnp.where(
                low, -pltpu.roll(x, LANES - ROPE // 2, 1), pltpu.roll(x, ROPE // 2, 1)
            )
            turned.append(x * cosine + other * sine)
        for p in range(dims.heads // 2):
            wide = plain[:, p * LANES : (p + 1) * LANES].astype(jnp.float32)
            rot = turned[2 * p * ROPE // LANES]
            for side in range(2):
                at = (2 * p + side) * ROPE % LANES
                mine_wide = (lane // NOPE) == side
                mine_rot = (lane // ROPE) == at // ROPE
                own = slice(side * rows_a, (side + 1) * rows_a)
                qs[p, own, :LANES] = jnp.where(mine_wide, wide, 0.0).astype(jnp.bfloat16)
                qs[p, own, LANES:] = jnp.where(mine_rot, rot, 0.0).astype(jnp.bfloat16)

    def key_values():
        l_wku.wait()
        l_wvu.wait()
        for j in range(n):
            keys[pl.ds(j * rows_a, rows_a), :] = jnp.dot(
                lat[j, :, : dims.rank], wku[...], preferred_element_type=jnp.float32
            ).astype(jnp.bfloat16)
            vals[pl.ds(j * rows_a, rows_a), :] = jnp.dot(
                lat[j, :, : dims.rank], wvu[...], preferred_element_type=jnp.float32
            ).astype(jnp.bfloat16)

    logit_scale = (NOPE + ROPE) ** (-0.5)

    def attend(p):
        at = slice(p * LANES, (p + 1) * LANES)
        contract = (((1,), (1,)), ((), ()))
        scores = []
        for j in range(n):
            block = jnp.concatenate(
                [keys[j * rows_a : (j + 1) * rows_a, at], lat[j, :, dims.rank :]], axis=1
            )
            scores.append(
                lax.dot_general(qs[p], block, contract, preferred_element_type=jnp.float32)
            )
        score = jnp.concatenate(scores, axis=1) * logit_scale
        shape = score.shape
        position = e * rows_a + lax.rem(lax.broadcasted_iota(jnp.int32, shape, 0), rows_a)
        allowed = lax.broadcasted_iota(jnp.int32, shape, 1) <= position
        masked = jnp.where(allowed, score, -1e30)
        top = jnp.max(masked, axis=1, keepdims=True)
        probs = jnp.where(allowed, jnp.exp(masked - top), 0.0)
        weight_sum = jnp.sum(probs, axis=1, keepdims=True)
        got = jnp.dot(probs.astype(jnp.bfloat16), vals[:, at], preferred_element_type=jnp.float32)
        got = got / weight_sum
        lane = lax.broadcasted_iota(jnp.int32, (rows_a, LANES), 1)
        att[:, at] = jnp.where(lane < VD, got[:rows_a], got[rows_a:]).astype(jnp.bfloat16)

    share_rows = rows_a // 4

    def rows_of(which):
        return pl.ds(pl.multiple_of(which * share_rows, share_rows), share_rows)

    am_copy = remote(am_send, am_recv, as_send, as_recv, tp=mate)
    ax_copy = remote(ax_send, ax_recv, at_send, at_recv, tp=across)

    def project():
        l_wo.wait()
        mixed[...] = jnp.dot(att[...], wo[...], preferred_element_type=jnp.float32).astype(
            jnp.bfloat16
        ).astype(jnp.float32)
        for place, mask in enumerate((1, 3)):
            am_send[place] = mixed[rows_of(quarter[mask]), :].astype(jnp.bfloat16)
        am_copy.start()

    def project_pair():
        am_copy.wait_recv()
        ax_send[...] = (mixed[rows_of(across), :] + am_recv[1].astype(jnp.float32)).astype(
            jnp.bfloat16
        )
        ax_copy.start()

    def project_end():
        ax_copy.wait_recv()
        out_a[...] = (
            mixed[rows_of(t), :]
            + am_recv[0].astype(jnp.float32)
            + ax_recv[...].astype(jnp.float32)
        ).astype(jnp.bfloat16)

    dispatch(1)
    dispatch(0)
    for m in range(2, n):
        dispatch(m)
    latents()
    l_wg.wait()
    l_wu.wait()
    l_wd.wait()
    order = list(range(1, n)) + [0]
    pairs_of_heads = dims.heads // 2
    extra = {0: [queries], 1: [latents_on], 2: [latents_over], 3: [latents_in, key_values]}
    for p in range(pairs_of_heads):
        extra.setdefault(4 + p, []).append(functools.partial(attend, p))
    extra.setdefault(4 + pairs_of_heads, []).append(project)
    extra.setdefault(5 + pairs_of_heads, []).append(project_pair)
    for i in range(max(n + 4, 6 + pairs_of_heads)):
        if i < n - 1:
            forward(order[i])
        if i == 0:
            relay(0)
        elif i <= n - 1:
            relay(order[i - 1])
        if 2 <= i < n + 2:
            expert(order[i - 2])
        if 3 <= i < n + 3:
            pair_sum(order[i - 3])
        if 4 <= i < n + 4:
            give_back(order[i - 4])
        for step in extra.get(i, []):
            step()
    for i, m in enumerate(order):
        combine(m, begin=i == 0)
    out_b[...] = total[...].astype(jnp.bfloat16)
    project_end()

    for m in range(n):
        if m:
            z_copy(m).wait_send()
            b_copy(m).wait_send()
        for make in (x_copy, c_copy, f_copy, p_copy, q_copy):
            make(m).wait_send()
    for k in range(quads):
        if k:
            lz_copy(k).wait_send()
        ly_copy(k).wait_send()
    for j in range(1, n):
        ld_copy(j, owner_of(j)).wait_send()
    am_copy.wait_send()
    ax_copy.wait_send()


@dataclasses.dataclass(frozen=True)
class Dims:
    n: int
    cap: int
    rows_a: int
    rows_b: int
    width: int
    rank: int
    heads: int


def fused_scratch(dims, args):
    (ta, _, wq, wqr, wl, wkr, _, wku, wvu, wo, tb, _, _, _, wg, wu, wd) = args
    n, cap, width, rows_a, rows_b = dims.n, dims.cap, dims.width, dims.rows_a, dims.rows_b
    model = ta.shape[1]
    bf, f32 = jnp.bfloat16, jnp.float32
    vmem = pltpu.VMEM
    copied = [vmem(a.shape, a.dtype) for a in (ta, wq, wqr, wl)]
    copied.append(vmem((wkr.shape[1], wkr.shape[0]), wkr.dtype))
    copied += [vmem(a.shape, a.dtype) for a in (wku, wvu, wo, tb, wg, wu, wd)]
    block = (cap, width)
    quarter_rows = rows_a // 4
    return copied, [
        vmem((rows_b, width), bf),
        vmem((LANES, rows_b), f32),
        vmem((rows_b, LANES), f32),
        vmem((rows_b, LANES), f32),
        vmem((n, *block), bf),
        vmem((4, n, *block), bf),
        vmem((n, 2, *block), f32),
        vmem((n, 2, *block), bf),
        vmem((n, 2, *block), bf),
        vmem((n, *block), bf),
        vmem((n, *block), bf),
        vmem((n, *block), bf),
        vmem((n, *block), bf),
        vmem((rows_b, width), f32),
        vmem((rows_a, model), bf),
        vmem((2 * LANES, model), bf),
        vmem((n, rows_a, dims.rank + LANES), bf),
        vmem((dims.heads // 2, 2 * rows_a, 2 * LANES), bf),
        vmem((n * rows_a, wku.shape[1]), bf),
        vmem((n * rows_a, wvu.shape[1]), bf),
        vmem((rows_a, wvu.shape[1]), bf),
        vmem((rows_a, model), f32),
        vmem((2, quarter_rows, model), bf),
        vmem((2, quarter_rows, model), bf),
        vmem((quarter_rows, model), bf),
        vmem((quarter_rows, model), bf),
    ]


def fused(dims, args):
    (ta, ag, wq, wqr, wl, wkr, lg, wku, wvu, wo, tb, fg, ids, wts, wg, wu, wd) = args
    copied, buffers = fused_scratch(dims, args)
    n = dims.n
    dma = pltpu.SemaphoreType.DMA
    sems = [dma((len(copied),))] + [dma((n,)) for _ in range(14)]
    sems += [dma((n,)) for _ in range(6)] + [dma, dma, dma, dma]
    near, far = rope_tables(dims.rows_a, n)
    anywhere = pl.BlockSpec(memory_space=pl.ANY)
    inside = pl.BlockSpec(memory_space=pltpu.VMEM)
    where = [
        anywhere, inside, anywhere, anywhere, anywhere, anywhere, inside, anywhere, anywhere,
        anywhere, anywhere, inside, inside, inside, anywhere, anywhere, anywhere, inside, inside,
    ]
    return pl.pallas_call(
        functools.partial(fused_kernel, dims),
        out_shape=(
            jax.ShapeDtypeStruct((dims.rows_a // 4, ta.shape[1]), jnp.bfloat16),
            jax.ShapeDtypeStruct((dims.rows_b, dims.width), jnp.bfloat16),
        ),
        in_specs=where,
        out_specs=(inside, inside),
        scratch_shapes=copied + buffers + sems,
        compiler_params=pltpu.CompilerParams(
            collective_id=0, has_side_effects=True, vmem_limit_bytes=VMEM_BYTES
        ),
        name="fused",
    )(
        ta, ag[None], wq, wqr, wl, wkr.T, lg[None], wku, wvu, wo, tb, fg[None], ids.T, wts.T,
        wg, wu, wd, jnp.asarray(near), jnp.asarray(far),
    )


def fused_dims(args):
    (ta, _, wq, wqr, wl, wkr, _, wku, wvu, wo, tb, _, ids, _, wg, _, wd) = args
    n, tp = lax.axis_size("ep"), lax.axis_size("tp")
    experts = wg.shape[0] * n
    dims = Dims(
        n=n,
        cap=2 * tb.shape[0] * ids.shape[1] // experts,
        rows_a=ta.shape[0],
        rows_b=tb.shape[0],
        width=tb.shape[1] // tp,
        rank=wl.shape[1],
        heads=wq.shape[1] // NOPE,
    )
    copied, buffers = fused_scratch(dims, args)
    held = sum(math.prod(b.shape) * b.dtype.itemsize for b in copied + buffers)
    good = (
        tp == 4
        and n % 2 == 0
        and wg.shape[0] == 1
        and ids.shape[1] == 2
        and experts <= LANES
        and dims.cap <= LANES
        and dims.cap % 16 == 0
        and held <= VMEM_BYTES * 7 // 8
    )
    return dims if good else None


def on_device(
    tokens_a,
    attn_gain,
    w_query,
    w_query_rot,
    w_latent,
    w_key_rot,
    latent_gain,
    w_key_up,
    w_value_up,
    w_output,
    tokens_b,
    ffn_gain,
    expert_ids,
    expert_weights,
    w_gate,
    w_up,
    w_down,
):
    args = (
        tokens_a, attn_gain, w_query, w_query_rot, w_latent, w_key_rot, latent_gain, w_key_up,
        w_value_up, w_output, tokens_b, ffn_gain, expert_ids, expert_weights, w_gate, w_up, w_down,
    )
    dims = fused_dims(args)
    if dims is not None:
        return fused(dims, args)
    expert_count = w_gate.shape[0] * lax.axis_size("ep")
    outgoing, before = dispatch_rows(tokens_b, ffn_gain, expert_ids, expert_count)
    mixed_a, arrived = attention_half(
        tokens_a,
        attn_gain,
        w_query,
        w_query_rot,
        w_latent,
        w_key_rot,
        latent_gain,
        w_key_up,
        w_value_up,
        w_output,
        outgoing,
    )
    mixed_b = expert_half(arrived, before, expert_ids, expert_weights, w_gate, w_up, w_down)
    return (mixed_a, mixed_b)


def solution(mesh):
    placed = (
        P("ep", None),
        P(),
        P(None, "tp"),
        P(None, "tp"),
        P(),
        P(),
        P(),
        P(None, "tp"),
        P(None, "tp"),
        P("tp", None),
        P("ep", None),
        P(),
        P("ep", None),
        P("ep", None),
        P("ep", None, "tp"),
        P("ep", None, "tp"),
        P("ep", "tp", None),
    )
    return jax.shard_map(
        on_device,
        mesh=mesh,
        in_specs=placed,
        out_specs=(P(("ep", "tp"), None), P("ep", "tp")),
        check_vma=False,
    )
```

```python
import dataclasses
import functools
import math

import jax
import jax.numpy as jnp
import numpy as np
from jax import lax
from jax.experimental import pallas as pl
from jax.experimental.pallas import tpu as pltpu
from jax.sharding import PartitionSpec as P

NOPE = 64
ROPE = 32
VD = 64
LANES = 128
VMEM_BYTES = 60 * 1024 * 1024


epsilon = 1e-06
rope_base = 10000.0


def normalize(matrix, gain):
    floats = matrix.astype(jnp.float32)
    scaled = floats * lax.rsqrt(jnp.mean(floats * floats, axis=-1, keepdims=True) + epsilon)
    return scaled * gain


def rotate(vectors, positions):
    rot_width = vectors.shape[-1]
    half_width = rot_width // 2
    inverse = rope_base ** (-(jnp.arange(half_width, dtype=jnp.float32) * 2.0) / rot_width)
    angles = positions.astype(jnp.float32)[:, None] * inverse[None, :]
    cosine = jnp.cos(angles)[:, None, :]
    sine_part = jnp.sin(angles)[:, None, :]
    first_half = vectors[..., :half_width]
    second_half = vectors[..., half_width:]
    return jnp.concatenate(
        [
            first_half * cosine - second_half * sine_part,
            first_half * sine_part + second_half * cosine,
        ],
        axis=-1,
    )


def attention_half(
    tokens_a,
    attn_gain,
    w_query,
    w_query_rot,
    w_latent,
    w_key_rot,
    latent_gain,
    w_key_up,
    w_value_up,
    w_output,
    outgoing,
):
    row_count = tokens_a.shape[0]
    head_count = w_query.shape[1] // NOPE
    offset = lax.axis_index("ep") * row_count
    positions = offset + jnp.arange(row_count, dtype=jnp.int32)
    normed = normalize(tokens_a, attn_gain).astype(jnp.bfloat16)
    query_plain = jnp.dot(normed, w_query, preferred_element_type=jnp.float32).astype(jnp.bfloat16)
    query_plain = query_plain.reshape(row_count, head_count, NOPE)
    turned = jnp.dot(normed, w_query_rot, preferred_element_type=jnp.float32).reshape(
        row_count, head_count, ROPE
    )
    query_rotated_rows = rotate(turned, positions).astype(jnp.bfloat16)
    latent = normalize(
        jnp.dot(normed, w_latent, preferred_element_type=jnp.float32), latent_gain
    ).astype(jnp.bfloat16)
    key_raw = jnp.dot(normed, w_key_rot, preferred_element_type=jnp.float32)[:, None, :]
    key_turned = rotate(key_raw, positions)[:, 0, :].astype(jnp.bfloat16)
    logit_scale = (NOPE + ROPE) ** (-0.5)
    outgoing, compact = lax.optimization_barrier(
        (outgoing, jnp.concatenate([latent, key_turned], axis=1))
    )
    joined = lax.all_gather(compact, "ep", axis=0, tiled=True)
    arrived = lax.all_to_all(outgoing, "ep", split_axis=0, concat_axis=0, tiled=True)
    pieces = (joined[:, : latent.shape[1]], joined[:, latent.shape[1] :])
    piece_keys = jnp.dot(pieces[0], w_key_up, preferred_element_type=jnp.float32).astype(
        jnp.bfloat16
    )
    piece_values = jnp.dot(pieces[0], w_value_up, preferred_element_type=jnp.float32).astype(
        jnp.bfloat16
    )
    key_count = piece_keys.shape[0]
    blocks = key_count // row_count
    key_blocks = piece_keys.reshape(blocks, row_count, head_count, NOPE)
    value_blocks = piece_values.reshape(blocks, row_count, head_count, VD)
    rotated_key_blocks = pieces[1].reshape(blocks, row_count, ROPE)
    score_matrix = (
        jnp.einsum("yvz,wrvz->yvwr", query_plain, key_blocks, preferred_element_type=jnp.float32)
        + jnp.einsum(
            "yjx,inx->yjin",
            query_rotated_rows,
            rotated_key_blocks,
            preferred_element_type=jnp.float32,
        )
    ) * logit_scale
    key_pos = jnp.arange(key_count, dtype=jnp.int32).reshape(blocks, row_count)
    allowed = key_pos[None, None, :, :] <= positions[:, None, None, None]
    masked = jnp.where(allowed, score_matrix, -1e30)
    block_max = jnp.max(masked, axis=-1)
    probs = jnp.where(allowed, jnp.exp(masked - block_max[..., None]), 0.0)
    block_total = jnp.sum(probs, axis=-1)
    block_out = jnp.einsum(
        "qhbk,bkhd->qhbd",
        probs.astype(jnp.bfloat16),
        value_blocks,
        preferred_element_type=jnp.float32,
    )
    run_max = jnp.full((row_count, head_count), -1e30, jnp.float32)
    new_max = jnp.maximum(run_max, jnp.max(block_max, axis=-1))
    new_factor = jnp.exp(block_max - new_max[..., None])
    new_total = jnp.sum(new_factor * block_total, axis=-1)
    new_out = jnp.sum(new_factor[..., None] * block_out, axis=2)
    attended = (
        (new_out / new_total[..., None]).astype(jnp.bfloat16).reshape(row_count, head_count * VD)
    )
    mixed = lax.psum_scatter(
        jnp.dot(attended, w_output, preferred_element_type=jnp.float32).astype(jnp.bfloat16),
        "tp",
        scatter_dimension=0,
        tiled=True,
    )
    return mixed, arrived


def dispatch_rows(tokens_b, ffn_gain, expert_ids, expert_count):
    row_count, width = tokens_b.shape
    top_count = expert_ids.shape[1]
    capacity = 2 * row_count * top_count // expert_count
    tp_count = lax.axis_size("tp")
    part_width = width // tp_count
    floats = tokens_b.astype(jnp.float32)
    factor = lax.rsqrt(jnp.mean(floats * floats, axis=-1, keepdims=True) + epsilon)
    start = lax.axis_index("tp") * part_width
    own = lax.dynamic_slice_in_dim(tokens_b, start, part_width, 1).astype(jnp.float32)
    own_gain = lax.dynamic_slice_in_dim(ffn_gain, start, part_width, 0)
    normed = (own * factor * own_gain).astype(jnp.bfloat16)
    experts = jnp.arange(expert_count, dtype=jnp.int32)
    slots = jnp.arange(capacity, dtype=jnp.int32)
    named = (expert_ids[:, :, None] == experts).any(axis=1)
    rows = jnp.arange(row_count, dtype=jnp.int32)
    earlier = (rows[:, None] > rows[None, :]).astype(jnp.bfloat16)
    before = jnp.dot(
        earlier, named.astype(jnp.bfloat16), preferred_element_type=jnp.float32
    ).astype(jnp.int32)
    slot_of = jnp.where(named, before, -1).T
    chosen = (slot_of[:, None, :] == slots[None, :, None]).astype(jnp.bfloat16)
    outgoing = jnp.dot(
        chosen.reshape(expert_count * capacity, row_count),
        normed,
        preferred_element_type=jnp.float32,
    ).astype(jnp.bfloat16)
    outgoing = outgoing.reshape(expert_count, capacity, part_width)
    return outgoing, before


def swap(block, distance, count):
    return lax.ppermute(block, "tp", [(i, i ^ distance) for i in range(count)])


def expert_half(arrived, before, expert_ids, expert_weights, w_gate, w_up, w_down):
    expert_count, capacity, part_width = arrived.shape
    tp_count = lax.axis_size("tp")
    top_count = expert_ids.shape[1]
    experts = jnp.arange(expert_count, dtype=jnp.int32)
    me = lax.axis_index("tp")
    blocks = {0: arrived.reshape(-1, part_width)}
    distance = tp_count // 2
    while distance:
        for mask in list(blocks):
            blocks[mask ^ distance] = swap(blocks[mask], distance, tp_count)
        distance //= 2
    gate_part = 0.0
    up_part = 0.0
    for mask, block in blocks.items():
        first = (me ^ mask) * part_width
        gate_rows = lax.dynamic_slice_in_dim(w_gate[0], first, part_width, 0)
        up_rows = lax.dynamic_slice_in_dim(w_up[0], first, part_width, 0)
        gate_part += jnp.dot(block, gate_rows, preferred_element_type=jnp.float32)
        up_part += jnp.dot(block, up_rows, preferred_element_type=jnp.float32)
    hidden = (jax.nn.silu(gate_part) * up_part).astype(jnp.bfloat16)
    parts = {}
    for mask in reversed(range(tp_count)):
        down_columns = lax.dynamic_slice_in_dim(w_down[0], (me ^ mask) * part_width, part_width, 1)
        parts[mask] = jnp.dot(hidden, down_columns, preferred_element_type=jnp.float32)
    distance = 1
    while distance < tp_count:
        for mask in [m for m in parts if m & distance]:
            came = swap(parts.pop(mask).astype(jnp.bfloat16), distance, tp_count)
            parts[mask ^ distance] += came.astype(jnp.float32)
        distance *= 2
    summed = parts[0].astype(jnp.bfloat16)
    returned = lax.all_to_all(
        summed.reshape(expert_count, capacity, part_width),
        "ep",
        split_axis=0,
        concat_axis=0,
        tiled=True,
    )
    shares = expert_weights / jnp.sum(expert_weights, axis=1, keepdims=True)
    table = returned.reshape(expert_count * capacity, part_width)
    total = 0.0
    for k in range(top_count):
        own_slot = jnp.sum(jnp.where(expert_ids[:, k : k + 1] == experts, before, 0), axis=1)
        target = expert_ids[:, k] * capacity + own_slot
        pick = (
            target[:, None] == jnp.arange(expert_count * capacity, dtype=jnp.int32)
        ).astype(jnp.bfloat16)
        picked = jnp.dot(pick, table, preferred_element_type=jnp.float32)
        total = total + picked * shares[:, k : k + 1]
    return total.astype(jnp.bfloat16)


DOUBLED = (1, 2, 3)


SCHEDULES = {
    8: (
        "D2", "D1", "enter", "S2", "S1", "D4", "S4", "own", "weights", "E0", "latents", "D5", "S5", "D6", "S6", "P0", "D7", "S7", "D3", "S3", "queries", "tables",
        "F2", "F1", "R1", "E1", "F4", "R2", "E2", "P1", "U1", "R4", "P2", "E4", "G0", "C0", "F5", "P4", "R5", "blank", "F6", "E5", "G4", "P5", "U2",
        "G1", "R6", "G2", "F3", "R3", "E6", "G5", "F7", "P6", "E3", "U3", "V0", "V1", "R7", "G6", "E7", "V2", "P7", "P3", "V3",
        "W", "keys", "A0", "A1", "G7", "A2", "A3", "project", "C1", "C4", "pair", "C5", "G3", "C6", "C2", "C3", "C7",
    )
}


def rope_tables(rows, blocks):
    half = ROPE // 2
    lane = np.arange(LANES) % ROPE
    inverse = rope_base ** (-((lane % half).astype(np.float64) * 2.0) / ROPE)
    near = np.arange(rows, dtype=np.float64)[:, None] * inverse[None, :]
    far = (np.arange(blocks, dtype=np.float64) * rows)[:, None] * inverse[None, :]
    pack = lambda v: np.asarray(v, np.float32)
    return pack(np.stack([np.cos(near), np.sin(near)])), pack(
        np.stack([np.cos(far), np.sin(far)], axis=1)
    )


def staged_as(step):
    @functools.wraps(step)
    def run(*given, **options):
        with jax.named_scope("_".join([step.__name__, *map(str, given)])):
            return step(*given, **options)

    return run


def fused_kernel(
    dims,
    ta_hbm, ag_hbm, wq_hbm, wqr_hbm, wl_hbm, wkr_hbm, lg_hbm, wku_hbm, wvu_hbm, wo_hbm,
    tb_hbm, fg_hbm, ids_hbm, wts_hbm, wg_hbm, wu_hbm, wd_hbm, near_hbm, far_hbm,
    out_a, out_b,
    ta, ag_ref, wq, wqr, wl, wkr, lg_ref, wku, wvu, wo,
    tb, fg_ref, ids_ref, wts_ref, wg, wu, wd, near_ref, far_ref,
    own_b, slot_t, slot_c, share_c, staged, wider, landed, part_keep, part_send, part_recv,
    pair_send, pair_recv, back_send, back_recv, total,
    normed_a, rot_w, lat, qs, keys, vals, att, mixed, am_send, am_recv, ax_send, ax_recv,
    load_sem, z_send, z_recv, x_send, x_recv, c_send, c_recv, f_send, f_recv,
    p_send, p_recv, q_send, q_recv, b_send, b_recv,
    lz_send, lz_recv, ly_send, ly_recv, ld_send, ld_recv, as_send, as_recv, at_send, at_recv,
):
    n, cap, rows_a, rows_b = dims.n, dims.cap, dims.rows_a, dims.rows_b
    width = dims.width
    e, t = lax.axis_index("ep"), lax.axis_index("tp")
    core = lax.rem(t, 2)
    mate, across = t + 1 - 2 * core, lax.rem(t + 2, 4)
    third = lax.rem(mate + 2, 4)
    quarter = (t, mate, across, third)
    floors, floor = n // 2, e // 2
    beside = e + 1 - 2 * lax.rem(e, 2)

    def partner(m):
        there, bit = e, 1
        while bit < n:
            if m & bit:
                there = there + bit - 2 * bit * lax.rem(e // bit, 2)
            bit *= 2
        return there

    def remote(src, dst, ssem, rsem, ep=None, tp=None):
        target = (e if ep is None else ep, t if tp is None else tp)
        return pltpu.make_async_remote_copy(
            src_ref=src, dst_ref=dst, send_sem=ssem, recv_sem=rsem,
            device_id=target, device_id_type=pl.DeviceIdType.MESH,
        )

    pairs = [
        (ids_hbm, ids_ref), (tb_hbm, tb), (fg_hbm, fg_ref), (ta_hbm, ta), (ag_hbm, ag_ref),
        (wl_hbm, wl), (wkr_hbm, wkr), (lg_hbm, lg_ref), (near_hbm, near_ref), (far_hbm, far_ref),
        (wg_hbm, wg), (wu_hbm, wu), (wd_hbm, wd), (wq_hbm, wq), (wqr_hbm, wqr),
        (wts_hbm, wts_ref), (wku_hbm, wku), (wvu_hbm, wvu), (wo_hbm, wo),
    ]
    loads = [pltpu.make_async_copy(s, d, load_sem.at[i]) for i, (s, d) in enumerate(pairs)]
    for load in loads:
        load.start()
    (l_ids, l_tb, l_fg, l_ta, l_ag, l_wl, l_wkr, l_lg, l_near, l_far) = loads[:10]
    (l_wg, l_wu, l_wd, l_wq, l_wqr, l_wts, l_wku, l_wvu, l_wo) = loads[10:]

    barrier = pltpu.get_barrier_semaphore()
    for k in range(1, n):
        pl.semaphore_signal(
            barrier, inc=1, device_id=(partner(k), t), device_id_type=pl.DeviceIdType.MESH
        )
    for peer in (mate, across):
        pl.semaphore_signal(
            barrier, inc=1, device_id=(e, peer), device_id_type=pl.DeviceIdType.MESH
        )

    def own_columns(which):
        return pl.ds(pl.multiple_of(which * width, width), width)

    with jax.named_scope("slots"):
        l_ids.wait()
        ids = ids_ref[...]
        sub = lax.broadcasted_iota(jnp.int32, (LANES, rows_b), 0)
        first, second = ids[0:1] == sub, ids[1:2] == sub
        named = jnp.logical_or(first, second)
        earlier = (
            lax.broadcasted_iota(jnp.int32, (rows_b, rows_b), 0)
            < lax.broadcasted_iota(jnp.int32, (rows_b, rows_b), 1)
        ).astype(jnp.float32).astype(jnp.bfloat16)
        before = jnp.dot(
            named.astype(jnp.float32).astype(jnp.bfloat16),
            earlier,
            preferred_element_type=jnp.float32,
        )
        slot = jnp.where(named, before, -1.0)
        slot_t[...] = slot

    with jax.named_scope("wait_tb"):
        l_tb.wait()
        l_fg.wait()
    with jax.named_scope("norm_b"):
        floats = tb[...].astype(jnp.float32)
        factor = lax.rsqrt(jnp.mean(floats * floats, axis=-1, keepdims=True) + epsilon)
        for mask in (0, 2):
            columns = own_columns(quarter[mask])
            own_b[mask] = (
                tb[:, columns].astype(jnp.float32) * factor * fg_ref[:, columns]
            ).astype(jnp.bfloat16)

    def z_copy(m):
        return remote(staged.at[m], landed.at[0, m], z_send.at[m], z_recv.at[m], ep=partner(m))

    def w_copy(m):
        return remote(
            wider.at[m], landed.at[2, m], x_send.at[m], x_recv.at[m], ep=partner(m)
        )

    def x_copy(m):
        return remote(landed.at[0, m], landed.at[2, m], x_send.at[m], x_recv.at[m], tp=across)

    def c_copy(m):
        return remote(landed.at[0, m], landed.at[1, m], c_send.at[m], c_recv.at[m], tp=mate)

    def f_copy(m):
        return remote(landed.at[2, m], landed.at[3, m], f_send.at[m], f_recv.at[m], tp=mate)

    def p_copy(m):
        return remote(part_send.at[m], part_recv.at[m], p_send.at[m], p_recv.at[m], tp=mate)

    def q_copy(m):
        return remote(pair_send.at[m], pair_recv.at[m], q_send.at[m], q_recv.at[m], tp=across)

    def b_copy(m):
        return remote(back_send.at[m], back_recv.at[m], b_send.at[m], b_recv.at[m], ep=partner(m))

    def chosen_for(m):
        row = slot_t[pl.ds(partner(m), 1), :]
        wanted = lax.broadcasted_iota(jnp.int32, (cap, rows_b), 0).astype(jnp.float32)
        return (row == wanted).astype(jnp.float32).astype(jnp.bfloat16)

    @staged_as
    def dispatch(m):
        chosen = chosen_for(m)
        staged[m] = jnp.dot(chosen, own_b[0], preferred_element_type=jnp.float32).astype(
            jnp.bfloat16
        )
        if m in DOUBLED:
            wider[m] = jnp.dot(chosen, own_b[2], preferred_element_type=jnp.float32).astype(
                jnp.bfloat16
            )

    @staged_as
    def send(m):
        z_copy(m).start()
        if m in DOUBLED:
            w_copy(m).start()

    @staged_as
    def enter():
        pl.semaphore_wait(barrier, n + 1)

    @staged_as
    def keep_own():
        floats = tb[...].astype(jnp.float32)
        factor = lax.rsqrt(jnp.mean(floats * floats, axis=-1, keepdims=True) + epsilon)
        for mask in (1, 3):
            columns = own_columns(quarter[mask])
            own_b[mask] = (
                tb[:, columns].astype(jnp.float32) * factor * fg_ref[:, columns]
            ).astype(jnp.bfloat16)
        chosen = chosen_for(0)
        for mask in range(4):
            landed[mask, 0] = jnp.dot(
                chosen, own_b[mask], preferred_element_type=jnp.float32
            ).astype(jnp.bfloat16)

    @staged_as
    def tables():
        slot_c[...] = slot_t[...].T
        ids = ids_ref[...]
        sub = lax.broadcasted_iota(jnp.int32, (LANES, rows_b), 0)
        l_wts.wait()
        weight = wts_ref[...]
        sum_weight = weight[0:1] + weight[1:2]
        share_c[...] = (
            jnp.where(ids[0:1] == sub, weight[0:1] / sum_weight, 0.0)
            + jnp.where(ids[1:2] == sub, weight[1:2] / sum_weight, 0.0)
        ).T

    @staged_as
    def forward(m):
        with jax.named_scope(f"wait_z_copy_{m}"):
            z_copy(m).wait_recv()
        if m not in DOUBLED:
            x_copy(m).start()
        c_copy(m).start()

    @staged_as
    def relay(m):
        with jax.named_scope(f"wait_x_copy_{m}"):
            (w_copy if m in DOUBLED else x_copy)(m).wait_recv()
        f_copy(m).start()

    @staged_as
    def expert(m):
        if m:
            with jax.named_scope(f"wait_c_copy_{m}"):
                c_copy(m).wait_recv()
            with jax.named_scope(f"wait_f_copy_{m}"):
                f_copy(m).wait_recv()
        gate = up = None
        for mask in range(4):
            at = own_columns(quarter[mask])
            block = landed[mask, m]
            g = jnp.dot(block, wg[0, at, :], preferred_element_type=jnp.float32)
            u = jnp.dot(block, wu[0, at, :], preferred_element_type=jnp.float32)
            gate, up = (g, u) if mask == 0 else (gate + g, up + u)
        hidden = (gate / (1.0 + jnp.exp(-gate)) * up).astype(jnp.bfloat16)
        for place, mask in enumerate((1, 3)):
            part_send[m, place] = jnp.dot(
                hidden, wd[0, :, own_columns(quarter[mask])], preferred_element_type=jnp.float32
            ).astype(jnp.bfloat16)
        p_copy(m).start()
        for place, mask in enumerate((0, 2)):
            part_keep[m, place] = jnp.dot(
                hidden, wd[0, :, own_columns(quarter[mask])], preferred_element_type=jnp.float32
            )

    @staged_as
    def pair_sum(m):
        with jax.named_scope(f"wait_p_copy_{m}"):
            p_copy(m).wait_recv()
        pair_send[m] = (part_keep[m, 1] + part_recv[m, 1].astype(jnp.float32)).astype(jnp.bfloat16)
        q_copy(m).start()
        part_keep[m, 0] = part_keep[m, 0] + part_recv[m, 0].astype(jnp.float32)

    @staged_as
    def give_back(m):
        with jax.named_scope(f"wait_q_copy_{m}"):
            q_copy(m).wait_recv()
        summed = (part_keep[m, 0] + pair_recv[m].astype(jnp.float32)).astype(jnp.bfloat16)
        if m:
            back_send[m] = summed
            b_copy(m).start()
        else:
            back_recv[0] = summed

    @staged_as
    def weights_in():
        l_wg.wait()
        l_wu.wait()
        l_wd.wait()

    @staged_as
    def combine(m):
        if m:
            with jax.named_scope(f"wait_b_copy_{m}"):
                b_copy(m).wait_recv()
        expert_at = partner(m)
        lane = lax.broadcasted_iota(jnp.int32, (rows_b, LANES), 1)
        here = lane == expert_at
        at = jnp.sum(jnp.where(here, slot_c[...], 0.0), axis=1, keepdims=True)
        share = jnp.sum(jnp.where(here, share_c[...], 0.0), axis=1, keepdims=True)
        wanted = lax.broadcasted_iota(jnp.int32, (rows_b, cap), 1).astype(jnp.float32)
        pick = (at == wanted).astype(jnp.float32).astype(jnp.bfloat16)
        picked = jnp.dot(pick, back_recv[m], preferred_element_type=jnp.float32) * share
        total[...] = total[...] + picked if m else picked

    half_rows = rows_a // 2
    mine = pl.ds(pl.multiple_of(core * half_rows, half_rows), half_rows)
    yours = pl.ds(pl.multiple_of((1 - core) * half_rows, half_rows), half_rows)

    def under(k, other=False):
        return lax.rem((beside if other else e) + n - 2 * k, n)

    def passing(block, ssem, rsem, ep=None, tp=None):
        return remote(block, block, ssem, rsem, ep, tp)

    def lz_copy(k):
        return passing(
            lat.at[under(k), mine], lz_send.at[k], lz_recv.at[k + 1], ep=lax.rem(e + 2, n)
        )

    def lz_arrival(k):
        return passing(
            lat.at[under(k), mine], lz_send.at[k], lz_recv.at[k], ep=lax.rem(e + 2, n)
        )

    def ly_copy(k):
        return passing(lat.at[under(k), mine], ly_send.at[k], ly_recv.at[k], ep=beside)

    def ly_arrival(k):
        return passing(lat.at[under(k, True), mine], ly_send.at[k], ly_recv.at[k], ep=beside)

    def ld_copy(k, other, rows=None):
        j = k + floors * other
        block = lat.at[under(k, other), mine if rows is None else rows]
        return passing(block, ld_send.at[j], ld_recv.at[j], tp=mate)

    rising = floor < floors - 1

    @staged_as
    def latents():
        l_ta.wait()
        l_ag.wait()
        rows = ta[...].astype(jnp.float32)
        scale = lax.rsqrt(jnp.mean(rows * rows, axis=-1, keepdims=True) + epsilon)
        normed_a[...] = (rows * scale * ag_ref[...]).astype(jnp.bfloat16)
        l_wl.wait()
        l_lg.wait()
        raw = jnp.dot(normed_a[...], wl[...], preferred_element_type=jnp.float32)
        scale = lax.rsqrt(jnp.mean(raw * raw, axis=-1, keepdims=True) + epsilon)
        lat[e, :, : dims.rank] = (raw * scale * lg_ref[...]).astype(jnp.bfloat16)
        l_wkr.wait()
        l_near.wait()
        l_far.wait()
        plain = wkr[...]
        swapped = jnp.concatenate([-plain[ROPE // 2 :], plain[: ROPE // 2]], axis=0)
        for copy in range(LANES // ROPE):
            rot_w[copy * ROPE : (copy + 1) * ROPE] = plain
            rot_w[LANES + copy * ROPE : LANES + (copy + 1) * ROPE] = swapped
        both = lax.dot_general(
            normed_a[...], rot_w[...], (((1,), (1,)), ((), ())), preferred_element_type=jnp.float32
        )
        cosine, sine = turn()
        lat[e, :, dims.rank :] = (both[:, :LANES] * cosine + both[:, LANES:] * sine).astype(
            jnp.bfloat16
        )
        pl.when(rising)(lz_copy(0).start)
        ly_copy(0).start()

    @staged_as
    def blank():
        for k in range(1, floors):

            @pl.when(floor + k < floors)
            def _():
                for side in range(2):
                    lat[2 * lax.rem(floor + k, floors) + side] = jnp.zeros(
                        lat.shape[1:], lat.dtype
                    )

    def turn():
        far = far_ref[e]
        cosine = near_ref[0] * far[0:1] - near_ref[1] * far[1:2]
        sine = near_ref[1] * far[0:1] + near_ref[0] * far[1:2]
        return cosine, sine

    @staged_as
    def latents_on(k):
        @pl.when(floor >= k)
        def _():
            with jax.named_scope("wait_lz"):
                lz_arrival(k).wait_recv()
            pl.when(rising)(lz_copy(k).start)
            ly_copy(k).start()
            ld_copy(k, False).start()

    @staged_as
    def latents_over(k):
        @pl.when(floor >= k)
        def _():
            with jax.named_scope("wait_ly"):
                ly_arrival(k).wait_recv()
            ld_copy(k, True).start()

    @staged_as
    def latents_in():
        for k in range(floors):

            @pl.when(floor >= k)
            def _():
                with jax.named_scope("wait_ld"):
                    if k:
                        ld_copy(k, False, yours).wait_recv()
                    ld_copy(k, True, yours).wait_recv()

    @staged_as
    def queries():
        l_wq.wait()
        l_wqr.wait()
        plain = jnp.dot(normed_a[...], wq[...], preferred_element_type=jnp.float32).astype(
            jnp.bfloat16
        )
        raw = jnp.dot(normed_a[...], wqr[...], preferred_element_type=jnp.float32)
        cosine, sine = turn()
        lane = lax.broadcasted_iota(jnp.int32, (rows_a, LANES), 1)
        low = lax.rem(lane, ROPE) < ROPE // 2
        turned = []
        for g in range(raw.shape[1] // LANES):
            x = raw[:, g * LANES : (g + 1) * LANES]
            other = jnp.where(
                low, -pltpu.roll(x, LANES - ROPE // 2, 1), pltpu.roll(x, ROPE // 2, 1)
            )
            turned.append(x * cosine + other * sine)
        for p in range(dims.heads // 2):
            wide = plain[:, p * LANES : (p + 1) * LANES].astype(jnp.float32)
            rot = turned[2 * p * ROPE // LANES]
            for side in range(2):
                at = (2 * p + side) * ROPE % LANES
                mine_wide = (lane // NOPE) == side
                mine_rot = (lane // ROPE) == at // ROPE
                own = slice(side * rows_a, (side + 1) * rows_a)
                qs[p, own, :LANES] = jnp.where(mine_wide, wide, 0.0).astype(jnp.bfloat16)
                qs[p, own, LANES:] = jnp.where(mine_rot, rot, 0.0).astype(jnp.bfloat16)

    @staged_as
    def key_values():
        l_wku.wait()
        l_wvu.wait()
        for j in range(n):
            keys[pl.ds(j * rows_a, rows_a), :] = jnp.dot(
                lat[j, :, : dims.rank], wku[...], preferred_element_type=jnp.float32
            ).astype(jnp.bfloat16)
            vals[pl.ds(j * rows_a, rows_a), :] = jnp.dot(
                lat[j, :, : dims.rank], wvu[...], preferred_element_type=jnp.float32
            ).astype(jnp.bfloat16)

    logit_scale = (NOPE + ROPE) ** (-0.5)

    @staged_as
    def attend(p):
        at = slice(p * LANES, (p + 1) * LANES)
        contract = (((1,), (1,)), ((), ()))
        scores = []
        for j in range(n):
            block = jnp.concatenate(
                [keys[j * rows_a : (j + 1) * rows_a, at], lat[j, :, dims.rank :]], axis=1
            )
            scores.append(
                lax.dot_general(qs[p], block, contract, preferred_element_type=jnp.float32)
            )
        score = jnp.concatenate(scores, axis=1) * logit_scale
        shape = score.shape
        position = e * rows_a + lax.rem(lax.broadcasted_iota(jnp.int32, shape, 0), rows_a)
        allowed = lax.broadcasted_iota(jnp.int32, shape, 1) <= position
        masked = jnp.where(allowed, score, -1e30)
        top = jnp.max(masked, axis=1, keepdims=True)
        probs = jnp.where(allowed, jnp.exp(masked - top), 0.0)
        weight_sum = jnp.sum(probs, axis=1, keepdims=True)
        got = jnp.dot(probs.astype(jnp.bfloat16), vals[:, at], preferred_element_type=jnp.float32)
        got = got / weight_sum
        lane = lax.broadcasted_iota(jnp.int32, (rows_a, LANES), 1)
        att[:, at] = jnp.where(lane < VD, got[:rows_a], got[rows_a:]).astype(jnp.bfloat16)

    share_rows = rows_a // 4

    def rows_of(which):
        return pl.ds(pl.multiple_of(which * share_rows, share_rows), share_rows)

    am_copy = remote(am_send, am_recv, as_send, as_recv, tp=mate)
    ax_copy = remote(ax_send, ax_recv, at_send, at_recv, tp=across)

    @staged_as
    def project():
        l_wo.wait()
        mixed[...] = jnp.dot(att[...], wo[...], preferred_element_type=jnp.float32).astype(
            jnp.bfloat16
        ).astype(jnp.float32)
        for place, mask in enumerate((1, 3)):
            am_send[place] = mixed[rows_of(quarter[mask]), :].astype(jnp.bfloat16)
        am_copy.start()

    @staged_as
    def project_pair():
        with jax.named_scope(f"wait_am_copy"):
            am_copy.wait_recv()
        ax_send[...] = (mixed[rows_of(across), :] + am_recv[1].astype(jnp.float32)).astype(
            jnp.bfloat16
        )
        ax_copy.start()

    @staged_as
    def project_end():
        with jax.named_scope(f"wait_ax_copy"):
            ax_copy.wait_recv()
        out_a[...] = (
            mixed[rows_of(t), :]
            + am_recv[0].astype(jnp.float32)
            + ax_recv[...].astype(jnp.float32)
        ).astype(jnp.bfloat16)

    stages = dict(
        D=dispatch, S=send, enter=enter, F=forward, R=relay, E=expert, P=pair_sum, G=give_back, C=combine,
        latents=latents, own=keep_own, queries=queries, tables=tables, blank=blank,
        U=latents_on, V=latents_over, W=latents_in, keys=key_values, A=attend,
        project=project, pair=project_pair, weights=weights_in,
    )
    for entry in SCHEDULES[n]:
        if entry in stages:
            stages[entry]()
        else:
            stages[entry[0]](int(entry[1:]))
    out_b[...] = total[...].astype(jnp.bfloat16)
    project_end()

    for m in range(1, n):
        for make in (z_copy, c_copy, f_copy, b_copy, w_copy if m in DOUBLED else x_copy):
            make(m).wait_send()
    for m in range(n):
        p_copy(m).wait_send()
        q_copy(m).wait_send()
    for k in range(floors):

        @pl.when(floor >= k)
        def _():
            pl.when(rising)(lz_copy(k).wait_send)
            ly_copy(k).wait_send()
            if k:
                ld_copy(k, False).wait_send()
            ld_copy(k, True).wait_send()

    am_copy.wait_send()
    ax_copy.wait_send()


@dataclasses.dataclass(frozen=True)
class Dims:
    n: int
    cap: int
    rows_a: int
    rows_b: int
    width: int
    rank: int
    heads: int


def fused_scratch(dims, args):
    ta, wku, wvu = args[0], args[7], args[8]
    n, cap, width, rows_a, rows_b = dims.n, dims.cap, dims.width, dims.rows_a, dims.rows_b
    model = ta.shape[1]
    bf, f32 = jnp.bfloat16, jnp.float32
    vmem = pltpu.VMEM
    copied = [vmem(a.shape, a.dtype) for a in args]
    block = (cap, width)
    quarter_rows = rows_a // 4
    return copied, [
        vmem((4, rows_b, width), bf),
        vmem((LANES, rows_b), f32),
        vmem((rows_b, LANES), f32),
        vmem((rows_b, LANES), f32),
        vmem((n, *block), bf),
        vmem((n, *block), bf),
        vmem((4, n, *block), bf),
        vmem((n, 2, *block), f32),
        vmem((n, 2, *block), bf),
        vmem((n, 2, *block), bf),
        vmem((n, *block), bf),
        vmem((n, *block), bf),
        vmem((n, *block), bf),
        vmem((n, *block), bf),
        vmem((rows_b, width), f32),
        vmem((rows_a, model), bf),
        vmem((2 * LANES, model), bf),
        vmem((n, rows_a, dims.rank + LANES), bf),
        vmem((dims.heads // 2, 2 * rows_a, 2 * LANES), bf),
        vmem((n * rows_a, wku.shape[1]), bf),
        vmem((n * rows_a, wvu.shape[1]), bf),
        vmem((rows_a, wvu.shape[1]), bf),
        vmem((rows_a, model), f32),
        vmem((2, quarter_rows, model), bf),
        vmem((2, quarter_rows, model), bf),
        vmem((quarter_rows, model), bf),
        vmem((quarter_rows, model), bf),
    ]


def fused(dims, args):
    ta = args[0]
    args = fused_operands(dims, args)
    copied, buffers = fused_scratch(dims, args)
    n = dims.n
    dma = pltpu.SemaphoreType.DMA
    sems = [dma((len(copied),))] + [dma((n,)) for _ in range(14)]
    sems += [dma((n + 1,)) for _ in range(6)] + [dma, dma, dma, dma]
    inside = pl.BlockSpec(memory_space=pltpu.VMEM)
    return pl.pallas_call(
        functools.partial(fused_kernel, dims),
        out_shape=(
            pltpu.VMEM((dims.rows_a // 4, ta.shape[1]), jnp.bfloat16),
            pltpu.VMEM((dims.rows_b, dims.width), jnp.bfloat16),
        ),
        in_specs=[pl.BlockSpec(memory_space=pltpu.HBM)] * len(args),
        out_specs=(inside, inside),
        scratch_shapes=copied + buffers + sems,
        compiler_params=pltpu.CompilerParams(
            collective_id=0, has_side_effects=True, vmem_limit_bytes=VMEM_BYTES
        ),
        name="fused",
    )(*args)


def fused_operands(dims, args):
    (ta, ag, wq, wqr, wl, wkr, lg, wku, wvu, wo, tb, fg, ids, wts, wg, wu, wd) = args
    near, far = rope_tables(dims.rows_a, dims.n)
    return (
        ta, ag[None], wq, wqr, wl, wkr.T, lg[None], wku, wvu, wo, tb, fg[None], ids.T, wts.T,
        wg, wu, wd, jnp.asarray(near), jnp.asarray(far),
    )


def fused_dims(args):
    (ta, _, wq, wqr, wl, wkr, _, wku, wvu, wo, tb, _, ids, _, wg, _, wd) = args
    n, tp = lax.axis_size("ep"), lax.axis_size("tp")
    experts = wg.shape[0] * n
    dims = Dims(
        n=n,
        cap=2 * tb.shape[0] * ids.shape[1] // experts,
        rows_a=ta.shape[0],
        rows_b=tb.shape[0],
        width=tb.shape[1] // tp,
        rank=wl.shape[1],
        heads=wq.shape[1] // NOPE,
    )
    copied, buffers = fused_scratch(dims, args)
    held = sum(math.prod(b.shape) * b.dtype.itemsize for b in copied + buffers)
    good = (
        n in SCHEDULES
        and tp == 4
        and n & (n - 1) == 0
        and dims.heads == 8
        and wg.shape[0] == 1
        and ids.shape[1] == 2
        and experts <= LANES
        and dims.cap <= LANES
        and dims.cap % 16 == 0
        and held <= VMEM_BYTES
    )
    return dims if good else None


def on_device(
    tokens_a,
    attn_gain,
    w_query,
    w_query_rot,
    w_latent,
    w_key_rot,
    latent_gain,
    w_key_up,
    w_value_up,
    w_output,
    tokens_b,
    ffn_gain,
    expert_ids,
    expert_weights,
    w_gate,
    w_up,
    w_down,
):
    args = (
        tokens_a, attn_gain, w_query, w_query_rot, w_latent, w_key_rot, latent_gain, w_key_up,
        w_value_up, w_output, tokens_b, ffn_gain, expert_ids, expert_weights, w_gate, w_up, w_down,
    )
    dims = fused_dims(args)
    if dims is not None:
        return fused(dims, args)
    expert_count = w_gate.shape[0] * lax.axis_size("ep")
    outgoing, before = dispatch_rows(tokens_b, ffn_gain, expert_ids, expert_count)
    mixed_a, arrived = attention_half(
        tokens_a,
        attn_gain,
        w_query,
        w_query_rot,
        w_latent,
        w_key_rot,
        latent_gain,
        w_key_up,
        w_value_up,
        w_output,
        outgoing,
    )
    mixed_b = expert_half(arrived, before, expert_ids, expert_weights, w_gate, w_up, w_down)
    return (mixed_a, mixed_b)


def solution(mesh):
    placed = (
        P("ep", None),
        P(),
        P(None, "tp"),
        P(None, "tp"),
        P(),
        P(),
        P(),
        P(None, "tp"),
        P(None, "tp"),
        P("tp", None),
        P("ep", None),
        P(),
        P("ep", None),
        P("ep", None),
        P("ep", None, "tp"),
        P("ep", None, "tp"),
        P("ep", "tp", None),
    )
    return jax.shard_map(
        on_device,
        mesh=mesh,
        in_specs=placed,
        out_specs=(P(("ep", "tp"), None), P("ep", "tp")),
        check_vma=False,
    )
```

```python
import dataclasses
import functools
import math

import jax
import jax.numpy as jnp
import numpy as np
from jax import lax
from jax.experimental import pallas as pl
from jax.experimental.pallas import tpu as pltpu
from jax.sharding import PartitionSpec as P

NOPE = 64
ROPE = 32
VD = 64
LANES = 128
VMEM_BYTES = 60 * 1024 * 1024


epsilon = 1e-06
rope_base = 10000.0


def normalize(matrix, gain):
    floats = matrix.astype(jnp.float32)
    scaled = floats * lax.rsqrt(jnp.mean(floats * floats, axis=-1, keepdims=True) + epsilon)
    return scaled * gain


def rotate(vectors, positions):
    rot_width = vectors.shape[-1]
    half_width = rot_width // 2
    inverse = rope_base ** (-(jnp.arange(half_width, dtype=jnp.float32) * 2.0) / rot_width)
    angles = positions.astype(jnp.float32)[:, None] * inverse[None, :]
    cosine = jnp.cos(angles)[:, None, :]
    sine_part = jnp.sin(angles)[:, None, :]
    first_half = vectors[..., :half_width]
    second_half = vectors[..., half_width:]
    return jnp.concatenate(
        [
            first_half * cosine - second_half * sine_part,
            first_half * sine_part + second_half * cosine,
        ],
        axis=-1,
    )


def attention_half(
    tokens_a,
    attn_gain,
    w_query,
    w_query_rot,
    w_latent,
    w_key_rot,
    latent_gain,
    w_key_up,
    w_value_up,
    w_output,
    outgoing,
):
    row_count = tokens_a.shape[0]
    head_count = w_query.shape[1] // NOPE
    offset = lax.axis_index("ep") * row_count
    positions = offset + jnp.arange(row_count, dtype=jnp.int32)
    normed = normalize(tokens_a, attn_gain).astype(jnp.bfloat16)
    query_plain = jnp.dot(normed, w_query, preferred_element_type=jnp.float32).astype(jnp.bfloat16)
    query_plain = query_plain.reshape(row_count, head_count, NOPE)
    turned = jnp.dot(normed, w_query_rot, preferred_element_type=jnp.float32).reshape(
        row_count, head_count, ROPE
    )
    query_rotated_rows = rotate(turned, positions).astype(jnp.bfloat16)
    latent = normalize(
        jnp.dot(normed, w_latent, preferred_element_type=jnp.float32), latent_gain
    ).astype(jnp.bfloat16)
    key_raw = jnp.dot(normed, w_key_rot, preferred_element_type=jnp.float32)[:, None, :]
    key_turned = rotate(key_raw, positions)[:, 0, :].astype(jnp.bfloat16)
    logit_scale = (NOPE + ROPE) ** (-0.5)
    outgoing, compact = lax.optimization_barrier(
        (outgoing, jnp.concatenate([latent, key_turned], axis=1))
    )
    joined = lax.all_gather(compact, "ep", axis=0, tiled=True)
    arrived = lax.all_to_all(outgoing, "ep", split_axis=0, concat_axis=0, tiled=True)
    pieces = (joined[:, : latent.shape[1]], joined[:, latent.shape[1] :])
    piece_keys = jnp.dot(pieces[0], w_key_up, preferred_element_type=jnp.float32).astype(
        jnp.bfloat16
    )
    piece_values = jnp.dot(pieces[0], w_value_up, preferred_element_type=jnp.float32).astype(
        jnp.bfloat16
    )
    key_count = piece_keys.shape[0]
    blocks = key_count // row_count
    key_blocks = piece_keys.reshape(blocks, row_count, head_count, NOPE)
    value_blocks = piece_values.reshape(blocks, row_count, head_count, VD)
    rotated_key_blocks = pieces[1].reshape(blocks, row_count, ROPE)
    score_matrix = (
        jnp.einsum("yvz,wrvz->yvwr", query_plain, key_blocks, preferred_element_type=jnp.float32)
        + jnp.einsum(
            "yjx,inx->yjin",
            query_rotated_rows,
            rotated_key_blocks,
            preferred_element_type=jnp.float32,
        )
    ) * logit_scale
    key_pos = jnp.arange(key_count, dtype=jnp.int32).reshape(blocks, row_count)
    allowed = key_pos[None, None, :, :] <= positions[:, None, None, None]
    masked = jnp.where(allowed, score_matrix, -1e30)
    block_max = jnp.max(masked, axis=-1)
    probs = jnp.where(allowed, jnp.exp(masked - block_max[..., None]), 0.0)
    block_total = jnp.sum(probs, axis=-1)
    block_out = jnp.einsum(
        "qhbk,bkhd->qhbd",
        probs.astype(jnp.bfloat16),
        value_blocks,
        preferred_element_type=jnp.float32,
    )
    run_max = jnp.full((row_count, head_count), -1e30, jnp.float32)
    new_max = jnp.maximum(run_max, jnp.max(block_max, axis=-1))
    new_factor = jnp.exp(block_max - new_max[..., None])
    new_total = jnp.sum(new_factor * block_total, axis=-1)
    new_out = jnp.sum(new_factor[..., None] * block_out, axis=2)
    attended = (
        (new_out / new_total[..., None]).astype(jnp.bfloat16).reshape(row_count, head_count * VD)
    )
    mixed = lax.psum_scatter(
        jnp.dot(attended, w_output, preferred_element_type=jnp.float32).astype(jnp.bfloat16),
        "tp",
        scatter_dimension=0,
        tiled=True,
    )
    return mixed, arrived


def dispatch_rows(tokens_b, ffn_gain, expert_ids, expert_count):
    row_count, width = tokens_b.shape
    top_count = expert_ids.shape[1]
    capacity = 2 * row_count * top_count // expert_count
    tp_count = lax.axis_size("tp")
    part_width = width // tp_count
    floats = tokens_b.astype(jnp.float32)
    factor = lax.rsqrt(jnp.mean(floats * floats, axis=-1, keepdims=True) + epsilon)
    start = lax.axis_index("tp") * part_width
    own = lax.dynamic_slice_in_dim(tokens_b, start, part_width, 1).astype(jnp.float32)
    own_gain = lax.dynamic_slice_in_dim(ffn_gain, start, part_width, 0)
    normed = (own * factor * own_gain).astype(jnp.bfloat16)
    experts = jnp.arange(expert_count, dtype=jnp.int32)
    slots = jnp.arange(capacity, dtype=jnp.int32)
    named = (expert_ids[:, :, None] == experts).any(axis=1)
    rows = jnp.arange(row_count, dtype=jnp.int32)
    earlier = (rows[:, None] > rows[None, :]).astype(jnp.bfloat16)
    before = jnp.dot(
        earlier, named.astype(jnp.bfloat16), preferred_element_type=jnp.float32
    ).astype(jnp.int32)
    slot_of = jnp.where(named, before, -1).T
    chosen = (slot_of[:, None, :] == slots[None, :, None]).astype(jnp.bfloat16)
    outgoing = jnp.dot(
        chosen.reshape(expert_count * capacity, row_count),
        normed,
        preferred_element_type=jnp.float32,
    ).astype(jnp.bfloat16)
    outgoing = outgoing.reshape(expert_count, capacity, part_width)
    return outgoing, before


def swap(block, distance, count):
    return lax.ppermute(block, "tp", [(i, i ^ distance) for i in range(count)])


def expert_half(arrived, before, expert_ids, expert_weights, w_gate, w_up, w_down):
    expert_count, capacity, part_width = arrived.shape
    tp_count = lax.axis_size("tp")
    top_count = expert_ids.shape[1]
    experts = jnp.arange(expert_count, dtype=jnp.int32)
    me = lax.axis_index("tp")
    blocks = {0: arrived.reshape(-1, part_width)}
    distance = tp_count // 2
    while distance:
        for mask in list(blocks):
            blocks[mask ^ distance] = swap(blocks[mask], distance, tp_count)
        distance //= 2
    gate_part = 0.0
    up_part = 0.0
    for mask, block in blocks.items():
        first = (me ^ mask) * part_width
        gate_rows = lax.dynamic_slice_in_dim(w_gate[0], first, part_width, 0)
        up_rows = lax.dynamic_slice_in_dim(w_up[0], first, part_width, 0)
        gate_part += jnp.dot(block, gate_rows, preferred_element_type=jnp.float32)
        up_part += jnp.dot(block, up_rows, preferred_element_type=jnp.float32)
    hidden = (jax.nn.silu(gate_part) * up_part).astype(jnp.bfloat16)
    parts = {}
    for mask in reversed(range(tp_count)):
        down_columns = lax.dynamic_slice_in_dim(w_down[0], (me ^ mask) * part_width, part_width, 1)
        parts[mask] = jnp.dot(hidden, down_columns, preferred_element_type=jnp.float32)
    distance = 1
    while distance < tp_count:
        for mask in [m for m in parts if m & distance]:
            came = swap(parts.pop(mask).astype(jnp.bfloat16), distance, tp_count)
            parts[mask ^ distance] += came.astype(jnp.float32)
        distance *= 2
    summed = parts[0].astype(jnp.bfloat16)
    returned = lax.all_to_all(
        summed.reshape(expert_count, capacity, part_width),
        "ep",
        split_axis=0,
        concat_axis=0,
        tiled=True,
    )
    shares = expert_weights / jnp.sum(expert_weights, axis=1, keepdims=True)
    table = returned.reshape(expert_count * capacity, part_width)
    total = 0.0
    for k in range(top_count):
        own_slot = jnp.sum(jnp.where(expert_ids[:, k : k + 1] == experts, before, 0), axis=1)
        target = expert_ids[:, k] * capacity + own_slot
        pick = (
            target[:, None] == jnp.arange(expert_count * capacity, dtype=jnp.int32)
        ).astype(jnp.bfloat16)
        picked = jnp.dot(pick, table, preferred_element_type=jnp.float32)
        total = total + picked * shares[:, k : k + 1]
    return total.astype(jnp.bfloat16)


DOUBLED = (1, 2, 3)
UNMIXED = (0, 1, 2)


SCHEDULES = {
    8: (
        "D2", "enter", "S2", "D1", "S1", "D4", "S4", "own", "weights", "E0", "latents", "D5", "S5", "D6", "S6", "P0", "D3", "S3", "queries", "tables",
        "F2", "F1", "R1", "E1", "F4", "R2", "E2", "P1", "U1", "D7", "S7", "P2", "R4", "C0", "E4", "F5", "P4", "F6", "blank", "R5", "E5", "G4", "P5", "F7", "U2",
        "R6", "F3", "R3", "E6", "G5", "E3", "P6", "C1", "U3", "V0", "V1", "P3", "R7", "V2", "E7", "C2", "G6", "V3", "P7", "N",
        "W", "keys", "G3", "A0", "A1", "G7", "A2", "A3", "project", "C4", "C5", "pair", "C6", "C3", "C7", "M",
    )
}


def rope_tables(rows, blocks):
    half = ROPE // 2
    lane = np.arange(LANES) % ROPE
    inverse = rope_base ** (-((lane % half).astype(np.float64) * 2.0) / ROPE)
    near = np.arange(rows, dtype=np.float64)[:, None] * inverse[None, :]
    far = (np.arange(blocks, dtype=np.float64) * rows)[:, None] * inverse[None, :]
    pack = lambda v: np.asarray(v, np.float32)
    return pack(np.stack([np.cos(near), np.sin(near)])), pack(
        np.stack([np.cos(far), np.sin(far)], axis=1)
    )


def staged_as(step):
    @functools.wraps(step)
    def run(*given, **options):
        with jax.named_scope("_".join([step.__name__, *map(str, given)])):
            return step(*given, **options)

    return run


def fused_kernel(
    dims,
    ta_hbm, ag_hbm, wq_hbm, wqr_hbm, wl_hbm, wkr_hbm, lg_hbm, wku_hbm, wvu_hbm, wo_hbm,
    tb_hbm, fg_hbm, ids_hbm, wts_hbm, wg_hbm, wu_hbm, wd_hbm, near_hbm, far_hbm,
    out_a, out_b,
    ta, ag_ref, wq, wqr, wl, wkr, lg_ref, wku, wvu, wo,
    tb, fg_ref, ids_ref, wts_ref, wg, wu, wd, near_ref, far_ref,
    own_b, slot_t, slot_c, share_c, staged, wider, landed, part_keep, part_send, part_recv,
    pair_send, pair_recv, back_send, back_recv, side_send, side_recv, total, total_side, near_send, near_recv,
    normed_a, rot_w, lat, qs, keys, vals, att, mixed, am_send, am_recv, ax_send, ax_recv,
    load_sem, z_send, z_recv, x_send, x_recv, c_send, c_recv, f_send, f_recv,
    p_send, p_recv, q_send, q_recv, b_send, b_recv, s_send, s_recv, n_send, n_recv,
    lz_send, lz_recv, ly_send, ly_recv, ld_send, ld_recv, as_send, as_recv, at_send, at_recv,
):
    n, cap, rows_a, rows_b = dims.n, dims.cap, dims.rows_a, dims.rows_b
    width = dims.width
    e, t = lax.axis_index("ep"), lax.axis_index("tp")
    core = lax.rem(t, 2)
    mate, across = t + 1 - 2 * core, lax.rem(t + 2, 4)
    third = lax.rem(mate + 2, 4)
    quarter = (t, mate, across, third)
    floors, floor = n // 2, e // 2
    beside = e + 1 - 2 * lax.rem(e, 2)

    def partner(m):
        there, bit = e, 1
        while bit < n:
            if m & bit:
                there = there + bit - 2 * bit * lax.rem(e // bit, 2)
            bit *= 2
        return there

    def remote(src, dst, ssem, rsem, ep=None, tp=None):
        target = (e if ep is None else ep, t if tp is None else tp)
        return pltpu.make_async_remote_copy(
            src_ref=src, dst_ref=dst, send_sem=ssem, recv_sem=rsem,
            device_id=target, device_id_type=pl.DeviceIdType.MESH,
        )

    pairs = [
        (ids_hbm, ids_ref), (tb_hbm, tb), (fg_hbm, fg_ref), (ta_hbm, ta), (ag_hbm, ag_ref),
        (wl_hbm, wl), (wkr_hbm, wkr), (lg_hbm, lg_ref), (near_hbm, near_ref), (far_hbm, far_ref),
        (wg_hbm, wg), (wu_hbm, wu), (wd_hbm, wd), (wq_hbm, wq), (wqr_hbm, wqr),
        (wts_hbm, wts_ref), (wku_hbm, wku), (wvu_hbm, wvu), (wo_hbm, wo),
    ]
    loads = [pltpu.make_async_copy(s, d, load_sem.at[i]) for i, (s, d) in enumerate(pairs)]
    for load in loads:
        load.start()
    (l_ids, l_tb, l_fg, l_ta, l_ag, l_wl, l_wkr, l_lg, l_near, l_far) = loads[:10]
    (l_wg, l_wu, l_wd, l_wq, l_wqr, l_wts, l_wku, l_wvu, l_wo) = loads[10:]

    barrier = pltpu.get_barrier_semaphore()
    for k in range(1, n):
        pl.semaphore_signal(
            barrier, inc=1, device_id=(partner(k), t), device_id_type=pl.DeviceIdType.MESH
        )
    for peer in (mate, across):
        pl.semaphore_signal(
            barrier, inc=1, device_id=(e, peer), device_id_type=pl.DeviceIdType.MESH
        )

    def own_columns(which):
        return pl.ds(pl.multiple_of(which * width, width), width)

    with jax.named_scope("slots"):
        l_ids.wait()
        ids = ids_ref[...]
        sub = lax.broadcasted_iota(jnp.int32, (LANES, rows_b), 0)
        first, second = ids[0:1] == sub, ids[1:2] == sub
        named = jnp.logical_or(first, second)
        earlier = (
            lax.broadcasted_iota(jnp.int32, (rows_b, rows_b), 0)
            < lax.broadcasted_iota(jnp.int32, (rows_b, rows_b), 1)
        ).astype(jnp.float32).astype(jnp.bfloat16)
        before = jnp.dot(
            named.astype(jnp.float32).astype(jnp.bfloat16),
            earlier,
            preferred_element_type=jnp.float32,
        )
        slot = jnp.where(named, before, -1.0)
        slot_t[...] = slot

    with jax.named_scope("wait_tb"):
        l_tb.wait()
        l_fg.wait()
    with jax.named_scope("norm_b"):
        floats = tb[...].astype(jnp.float32)
        factor = lax.rsqrt(jnp.mean(floats * floats, axis=-1, keepdims=True) + epsilon)
        for mask in (0, 2):
            columns = own_columns(quarter[mask])
            own_b[mask] = (
                tb[:, columns].astype(jnp.float32) * factor * fg_ref[:, columns]
            ).astype(jnp.bfloat16)

    def z_copy(m):
        return remote(staged.at[m], landed.at[0, m], z_send.at[m], z_recv.at[m], ep=partner(m))

    def w_copy(m):
        return remote(
            wider.at[m], landed.at[2, m], x_send.at[m], x_recv.at[m], ep=partner(m)
        )

    def x_copy(m):
        return remote(landed.at[0, m], landed.at[2, m], x_send.at[m], x_recv.at[m], tp=across)

    def c_copy(m):
        return remote(landed.at[0, m], landed.at[1, m], c_send.at[m], c_recv.at[m], tp=mate)

    def f_copy(m):
        return remote(landed.at[2, m], landed.at[3, m], f_send.at[m], f_recv.at[m], tp=mate)

    def p_copy(m):
        return remote(part_send.at[m], part_recv.at[m], p_send.at[m], p_recv.at[m], tp=mate)

    def q_copy(m):
        return remote(pair_send.at[m], pair_recv.at[m], q_send.at[m], q_recv.at[m], tp=across)

    def b_copy(m):
        return remote(back_send.at[m], back_recv.at[m], b_send.at[m], b_recv.at[m], ep=partner(m))

    def s_copy(m):
        return remote(
            side_send.at[m], side_recv.at[m], s_send.at[m], s_recv.at[m], ep=partner(m)
        )

    def chosen_for(m):
        row = slot_t[pl.ds(partner(m), 1), :]
        wanted = lax.broadcasted_iota(jnp.int32, (cap, rows_b), 0).astype(jnp.float32)
        return (row == wanted).astype(jnp.float32).astype(jnp.bfloat16)

    @staged_as
    def dispatch(m):
        chosen = chosen_for(m)
        staged[m] = jnp.dot(chosen, own_b[0], preferred_element_type=jnp.float32).astype(
            jnp.bfloat16
        )
        if m in DOUBLED:
            wider[m] = jnp.dot(chosen, own_b[2], preferred_element_type=jnp.float32).astype(
                jnp.bfloat16
            )

    @staged_as
    def send(m):
        z_copy(m).start()
        if m in DOUBLED:
            w_copy(m).start()

    @staged_as
    def enter():
        pl.semaphore_wait(barrier, n + 1)

    @staged_as
    def keep_own():
        floats = tb[...].astype(jnp.float32)
        factor = lax.rsqrt(jnp.mean(floats * floats, axis=-1, keepdims=True) + epsilon)
        for mask in (1, 3):
            columns = own_columns(quarter[mask])
            own_b[mask] = (
                tb[:, columns].astype(jnp.float32) * factor * fg_ref[:, columns]
            ).astype(jnp.bfloat16)
        chosen = chosen_for(0)
        for mask in range(4):
            landed[mask, 0] = jnp.dot(
                chosen, own_b[mask], preferred_element_type=jnp.float32
            ).astype(jnp.bfloat16)

    @staged_as
    def tables():
        slot_c[...] = slot_t[...].T
        ids = ids_ref[...]
        sub = lax.broadcasted_iota(jnp.int32, (LANES, rows_b), 0)
        l_wts.wait()
        weight = wts_ref[...]
        sum_weight = weight[0:1] + weight[1:2]
        share_c[...] = (
            jnp.where(ids[0:1] == sub, weight[0:1] / sum_weight, 0.0)
            + jnp.where(ids[1:2] == sub, weight[1:2] / sum_weight, 0.0)
        ).T

    @staged_as
    def forward(m):
        with jax.named_scope(f"wait_z_copy_{m}"):
            z_copy(m).wait_recv()
        if m not in DOUBLED:
            x_copy(m).start()
        c_copy(m).start()

    @staged_as
    def relay(m):
        with jax.named_scope(f"wait_x_copy_{m}"):
            (w_copy if m in DOUBLED else x_copy)(m).wait_recv()
        f_copy(m).start()

    @staged_as
    def expert(m):
        if m:
            with jax.named_scope(f"wait_c_copy_{m}"):
                c_copy(m).wait_recv()
            with jax.named_scope(f"wait_f_copy_{m}"):
                f_copy(m).wait_recv()
        gate = up = None
        for mask in range(4):
            at = own_columns(quarter[mask])
            block = landed[mask, m]
            g = jnp.dot(block, wg[0, at, :], preferred_element_type=jnp.float32)
            u = jnp.dot(block, wu[0, at, :], preferred_element_type=jnp.float32)
            gate, up = (g, u) if mask == 0 else (gate + g, up + u)
        hidden = (gate / (1.0 + jnp.exp(-gate)) * up).astype(jnp.bfloat16)
        for place, mask in enumerate((1, 3)):
            part_send[m, place] = jnp.dot(
                hidden, wd[0, :, own_columns(quarter[mask])], preferred_element_type=jnp.float32
            ).astype(jnp.bfloat16)
        p_copy(m).start()
        for place, mask in enumerate((0, 2)):
            part_keep[m, place] = jnp.dot(
                hidden, wd[0, :, own_columns(quarter[mask])], preferred_element_type=jnp.float32
            )

    @staged_as
    def pair_sum(m):
        with jax.named_scope(f"wait_p_copy_{m}"):
            p_copy(m).wait_recv()
        side = (part_keep[m, 1] + part_recv[m, 1].astype(jnp.float32)).astype(jnp.bfloat16)
        if m in UNMIXED:
            own = (part_keep[m, 0] + part_recv[m, 0].astype(jnp.float32)).astype(jnp.bfloat16)
            if m:
                back_send[m] = own
                b_copy(m).start()
                side_send[m] = side
                s_copy(m).start()
            else:
                back_recv[0] = own
                side_recv[0] = side
            return
        pair_send[m] = side
        q_copy(m).start()
        part_keep[m, 0] = part_keep[m, 0] + part_recv[m, 0].astype(jnp.float32)

    @staged_as
    def give_back(m):
        with jax.named_scope(f"wait_q_copy_{m}"):
            q_copy(m).wait_recv()
        summed = (part_keep[m, 0] + pair_recv[m].astype(jnp.float32)).astype(jnp.bfloat16)
        if m:
            back_send[m] = summed
            b_copy(m).start()
        else:
            back_recv[0] = summed

    @staged_as
    def weights_in():
        l_wg.wait()
        l_wu.wait()
        l_wd.wait()

    @staged_as
    def combine(m):
        if m:
            with jax.named_scope(f"wait_b_copy_{m}"):
                b_copy(m).wait_recv()
        expert_at = partner(m)
        lane = lax.broadcasted_iota(jnp.int32, (rows_b, LANES), 1)
        here = lane == expert_at
        at = jnp.sum(jnp.where(here, slot_c[...], 0.0), axis=1, keepdims=True)
        share = jnp.sum(jnp.where(here, share_c[...], 0.0), axis=1, keepdims=True)
        wanted = lax.broadcasted_iota(jnp.int32, (rows_b, cap), 1).astype(jnp.float32)
        pick = (at == wanted).astype(jnp.float32).astype(jnp.bfloat16)
        picked = jnp.dot(pick, back_recv[m], preferred_element_type=jnp.float32) * share
        total[...] = total[...] + picked if m else picked
        if m in UNMIXED:
            if m:
                with jax.named_scope(f"wait_s_copy_{m}"):
                    s_copy(m).wait_recv()
            picked = jnp.dot(pick, side_recv[m], preferred_element_type=jnp.float32) * share
            total_side[...] = total_side[...] + picked if m else picked

    n_copy = remote(near_send, near_recv, n_send, n_recv, tp=across)

    @staged_as
    def near_out():
        near_send[...] = total_side[...].astype(jnp.bfloat16)
        n_copy.start()

    @staged_as
    def near_in():
        with jax.named_scope("wait_n_copy"):
            n_copy.wait_recv()
        total[...] = total[...] + near_recv[...].astype(jnp.float32)

    half_rows = rows_a // 2
    mine = pl.ds(pl.multiple_of(core * half_rows, half_rows), half_rows)
    yours = pl.ds(pl.multiple_of((1 - core) * half_rows, half_rows), half_rows)

    def under(k, other=False):
        return lax.rem((beside if other else e) + n - 2 * k, n)

    def passing(block, ssem, rsem, ep=None, tp=None):
        return remote(block, block, ssem, rsem, ep, tp)

    def lz_copy(k):
        return passing(
            lat.at[under(k), mine], lz_send.at[k], lz_recv.at[k + 1], ep=lax.rem(e + 2, n)
        )

    def lz_far():
        return passing(
            lat.at[under(1), mine], lz_send.at[2], lz_recv.at[3], ep=lax.rem(e + 4, n)
        )

    def lz_arrival(k):
        return passing(
            lat.at[under(k), mine], lz_send.at[k], lz_recv.at[k], ep=lax.rem(e + 2, n)
        )

    def ly_copy(k):
        return passing(lat.at[under(k), mine], ly_send.at[k], ly_recv.at[k], ep=beside)

    def ly_arrival(k):
        return passing(lat.at[under(k, True), mine], ly_send.at[k], ly_recv.at[k], ep=beside)

    def ld_copy(k, other, rows=None):
        j = k + floors * other
        block = lat.at[under(k, other), mine if rows is None else rows]
        return passing(block, ld_send.at[j], ld_recv.at[j], tp=mate)

    rising = floor < floors - 1
    rising_far = floor < floors - 2

    @staged_as
    def latents():
        l_ta.wait()
        l_ag.wait()
        rows = ta[...].astype(jnp.float32)
        scale = lax.rsqrt(jnp.mean(rows * rows, axis=-1, keepdims=True) + epsilon)
        normed_a[...] = (rows * scale * ag_ref[...]).astype(jnp.bfloat16)
        l_wl.wait()
        l_lg.wait()
        raw = jnp.dot(normed_a[...], wl[...], preferred_element_type=jnp.float32)
        scale = lax.rsqrt(jnp.mean(raw * raw, axis=-1, keepdims=True) + epsilon)
        lat[e, :, : dims.rank] = (raw * scale * lg_ref[...]).astype(jnp.bfloat16)
        l_wkr.wait()
        l_near.wait()
        l_far.wait()
        plain = wkr[...]
        swapped = jnp.concatenate([-plain[ROPE // 2 :], plain[: ROPE // 2]], axis=0)
        for copy in range(LANES // ROPE):
            rot_w[copy * ROPE : (copy + 1) * ROPE] = plain
            rot_w[LANES + copy * ROPE : LANES + (copy + 1) * ROPE] = swapped
        both = lax.dot_general(
            normed_a[...], rot_w[...], (((1,), (1,)), ((), ())), preferred_element_type=jnp.float32
        )
        cosine, sine = turn()
        lat[e, :, dims.rank :] = (both[:, :LANES] * cosine + both[:, LANES:] * sine).astype(
            jnp.bfloat16
        )
        pl.when(rising)(lz_copy(0).start)
        ly_copy(0).start()

    @staged_as
    def blank():
        for k in range(1, floors):

            @pl.when(floor + k < floors)
            def _():
                for side in range(2):
                    lat[2 * lax.rem(floor + k, floors) + side] = jnp.zeros(
                        lat.shape[1:], lat.dtype
                    )

    def turn():
        far = far_ref[e]
        cosine = near_ref[0] * far[0:1] - near_ref[1] * far[1:2]
        sine = near_ref[1] * far[0:1] + near_ref[0] * far[1:2]
        return cosine, sine

    @staged_as
    def latents_on(k):
        @pl.when(floor >= k)
        def _():
            with jax.named_scope("wait_lz"):
                lz_arrival(k).wait_recv()
            if k == 1:
                pl.when(rising)(lz_copy(1).start)
                pl.when(rising_far)(lz_far().start)
            ly_copy(k).start()
            ld_copy(k, False).start()

    @staged_as
    def latents_over(k):
        @pl.when(floor >= k)
        def _():
            with jax.named_scope("wait_ly"):
                ly_arrival(k).wait_recv()
            ld_copy(k, True).start()

    @staged_as
    def latents_in():
        for k in range(floors):

            @pl.when(floor >= k)
            def _():
                with jax.named_scope("wait_ld"):
                    if k:
                        ld_copy(k, False, yours).wait_recv()
                    ld_copy(k, True, yours).wait_recv()

    @staged_as
    def queries():
        l_wq.wait()
        l_wqr.wait()
        plain = jnp.dot(normed_a[...], wq[...], preferred_element_type=jnp.float32).astype(
            jnp.bfloat16
        )
        raw = jnp.dot(normed_a[...], wqr[...], preferred_element_type=jnp.float32)
        cosine, sine = turn()
        lane = lax.broadcasted_iota(jnp.int32, (rows_a, LANES), 1)
        low = lax.rem(lane, ROPE) < ROPE // 2
        turned = []
        for g in range(raw.shape[1] // LANES):
            x = raw[:, g * LANES : (g + 1) * LANES]
            other = jnp.where(
                low, -pltpu.roll(x, LANES - ROPE // 2, 1), pltpu.roll(x, ROPE // 2, 1)
            )
            turned.append(x * cosine + other * sine)
        for p in range(dims.heads // 2):
            wide = plain[:, p * LANES : (p + 1) * LANES].astype(jnp.float32)
            rot = turned[2 * p * ROPE // LANES]
            for side in range(2):
                at = (2 * p + side) * ROPE % LANES
                mine_wide = (lane // NOPE) == side
                mine_rot = (lane // ROPE) == at // ROPE
                own = slice(side * rows_a, (side + 1) * rows_a)
                qs[p, own, :LANES] = jnp.where(mine_wide, wide, 0.0).astype(jnp.bfloat16)
                qs[p, own, LANES:] = jnp.where(mine_rot, rot, 0.0).astype(jnp.bfloat16)

    @staged_as
    def key_values():
        l_wku.wait()
        l_wvu.wait()
        for j in range(n):
            keys[pl.ds(j * rows_a, rows_a), :] = jnp.dot(
                lat[j, :, : dims.rank], wku[...], preferred_element_type=jnp.float32
            ).astype(jnp.bfloat16)
            vals[pl.ds(j * rows_a, rows_a), :] = jnp.dot(
                lat[j, :, : dims.rank], wvu[...], preferred_element_type=jnp.float32
            ).astype(jnp.bfloat16)

    logit_scale = (NOPE + ROPE) ** (-0.5)

    @staged_as
    def attend(p):
        at = slice(p * LANES, (p + 1) * LANES)
        contract = (((1,), (1,)), ((), ()))
        scores = []
        for j in range(n):
            block = jnp.concatenate(
                [keys[j * rows_a : (j + 1) * rows_a, at], lat[j, :, dims.rank :]], axis=1
            )
            scores.append(
                lax.dot_general(qs[p], block, contract, preferred_element_type=jnp.float32)
            )
        score = jnp.concatenate(scores, axis=1) * logit_scale
        shape = score.shape
        position = e * rows_a + lax.rem(lax.broadcasted_iota(jnp.int32, shape, 0), rows_a)
        allowed = lax.broadcasted_iota(jnp.int32, shape, 1) <= position
        masked = jnp.where(allowed, score, -1e30)
        top = jnp.max(masked, axis=1, keepdims=True)
        probs = jnp.where(allowed, jnp.exp(masked - top), 0.0)
        weight_sum = jnp.sum(probs, axis=1, keepdims=True)
        got = jnp.dot(probs.astype(jnp.bfloat16), vals[:, at], preferred_element_type=jnp.float32)
        got = got / weight_sum
        lane = lax.broadcasted_iota(jnp.int32, (rows_a, LANES), 1)
        att[:, at] = jnp.where(lane < VD, got[:rows_a], got[rows_a:]).astype(jnp.bfloat16)

    share_rows = rows_a // 4

    def rows_of(which):
        return pl.ds(pl.multiple_of(which * share_rows, share_rows), share_rows)

    am_copy = remote(am_send, am_recv, as_send, as_recv, tp=mate)
    ax_copy = remote(ax_send, ax_recv, at_send, at_recv, tp=across)

    @staged_as
    def project():
        l_wo.wait()
        mixed[...] = jnp.dot(att[...], wo[...], preferred_element_type=jnp.float32).astype(
            jnp.bfloat16
        ).astype(jnp.float32)
        for place, mask in enumerate((1, 3)):
            am_send[place] = mixed[rows_of(quarter[mask]), :].astype(jnp.bfloat16)
        am_copy.start()

    @staged_as
    def project_pair():
        with jax.named_scope(f"wait_am_copy"):
            am_copy.wait_recv()
        ax_send[...] = (mixed[rows_of(across), :] + am_recv[1].astype(jnp.float32)).astype(
            jnp.bfloat16
        )
        ax_copy.start()

    @staged_as
    def project_end():
        with jax.named_scope(f"wait_ax_copy"):
            ax_copy.wait_recv()
        out_a[...] = (
            mixed[rows_of(t), :]
            + am_recv[0].astype(jnp.float32)
            + ax_recv[...].astype(jnp.float32)
        ).astype(jnp.bfloat16)

    stages = dict(
        D=dispatch, S=send, enter=enter, F=forward, R=relay, E=expert, P=pair_sum, G=give_back, C=combine,
        latents=latents, own=keep_own, queries=queries, tables=tables, blank=blank,
        U=latents_on, V=latents_over, W=latents_in, keys=key_values, A=attend,
        N=near_out, M=near_in, project=project, pair=project_pair, weights=weights_in,
    )
    for entry in SCHEDULES[n]:
        if entry in stages:
            stages[entry]()
        else:
            stages[entry[0]](int(entry[1:]))
    out_b[...] = total[...].astype(jnp.bfloat16)
    project_end()

    for m in range(1, n):
        for make in (z_copy, c_copy, f_copy, b_copy, w_copy if m in DOUBLED else x_copy):
            make(m).wait_send()
    for m in range(n):
        p_copy(m).wait_send()
        if m not in UNMIXED:
            q_copy(m).wait_send()
        elif m:
            s_copy(m).wait_send()
    n_copy.wait_send()
    for k in range(floors):

        @pl.when(floor >= k)
        def _():
            if k <= 1:
                pl.when(rising)(lz_copy(k).wait_send)
            if k == 1:
                pl.when(rising_far)(lz_far().wait_send)
            ly_copy(k).wait_send()
            if k:
                ld_copy(k, False).wait_send()
            ld_copy(k, True).wait_send()

    am_copy.wait_send()
    ax_copy.wait_send()


@dataclasses.dataclass(frozen=True)
class Dims:
    n: int
    cap: int
    rows_a: int
    rows_b: int
    width: int
    rank: int
    heads: int


def fused_scratch(dims, args):
    ta, wku, wvu = args[0], args[7], args[8]
    n, cap, width, rows_a, rows_b = dims.n, dims.cap, dims.width, dims.rows_a, dims.rows_b
    model = ta.shape[1]
    bf, f32 = jnp.bfloat16, jnp.float32
    vmem = pltpu.VMEM
    copied = [vmem(a.shape, a.dtype) for a in args]
    block = (cap, width)
    quarter_rows = rows_a // 4
    return copied, [
        vmem((4, rows_b, width), bf),
        vmem((LANES, rows_b), f32),
        vmem((rows_b, LANES), f32),
        vmem((rows_b, LANES), f32),
        vmem((n, *block), bf),
        vmem((n, *block), bf),
        vmem((4, n, *block), bf),
        vmem((n, 2, *block), f32),
        vmem((n, 2, *block), bf),
        vmem((n, 2, *block), bf),
        vmem((n, *block), bf),
        vmem((n, *block), bf),
        vmem((n, *block), bf),
        vmem((n, *block), bf),
        vmem((n // 2, *block), bf),
        vmem((n // 2, *block), bf),
        vmem((rows_b, width), f32),
        vmem((rows_b, width), f32),
        vmem((rows_b, width), bf),
        vmem((rows_b, width), bf),
        vmem((rows_a, model), bf),
        vmem((2 * LANES, model), bf),
        vmem((n, rows_a, dims.rank + LANES), bf),
        vmem((dims.heads // 2, 2 * rows_a, 2 * LANES), bf),
        vmem((n * rows_a, wku.shape[1]), bf),
        vmem((n * rows_a, wvu.shape[1]), bf),
        vmem((rows_a, wvu.shape[1]), bf),
        vmem((rows_a, model), f32),
        vmem((2, quarter_rows, model), bf),
        vmem((2, quarter_rows, model), bf),
        vmem((quarter_rows, model), bf),
        vmem((quarter_rows, model), bf),
    ]


def fused(dims, args):
    ta = args[0]
    args = fused_operands(dims, args)
    copied, buffers = fused_scratch(dims, args)
    n = dims.n
    dma = pltpu.SemaphoreType.DMA
    sems = [dma((len(copied),))] + [dma((n,)) for _ in range(16)] + [dma, dma]
    sems += [dma((n + 1,)) for _ in range(6)] + [dma, dma, dma, dma]
    inside = pl.BlockSpec(memory_space=pltpu.VMEM)
    return pl.pallas_call(
        functools.partial(fused_kernel, dims),
        out_shape=(
            pltpu.VMEM((dims.rows_a // 4, ta.shape[1]), jnp.bfloat16),
            pltpu.VMEM((dims.rows_b, dims.width), jnp.bfloat16),
        ),
        in_specs=[pl.BlockSpec(memory_space=pltpu.HBM)] * len(args),
        out_specs=(inside, inside),
        scratch_shapes=copied + buffers + sems,
        compiler_params=pltpu.CompilerParams(
            collective_id=0, has_side_effects=True, vmem_limit_bytes=VMEM_BYTES
        ),
        name="fused",
    )(*args)


def fused_operands(dims, args):
    (ta, ag, wq, wqr, wl, wkr, lg, wku, wvu, wo, tb, fg, ids, wts, wg, wu, wd) = args
    near, far = rope_tables(dims.rows_a, dims.n)
    return (
        ta, ag[None], wq, wqr, wl, wkr.T, lg[None], wku, wvu, wo, tb, fg[None], ids.T, wts.T,
        wg, wu, wd, jnp.asarray(near), jnp.asarray(far),
    )


def fused_dims(args):
    (ta, _, wq, wqr, wl, wkr, _, wku, wvu, wo, tb, _, ids, _, wg, _, wd) = args
    n, tp = lax.axis_size("ep"), lax.axis_size("tp")
    experts = wg.shape[0] * n
    dims = Dims(
        n=n,
        cap=2 * tb.shape[0] * ids.shape[1] // experts,
        rows_a=ta.shape[0],
        rows_b=tb.shape[0],
        width=tb.shape[1] // tp,
        rank=wl.shape[1],
        heads=wq.shape[1] // NOPE,
    )
    copied, buffers = fused_scratch(dims, args)
    held = sum(math.prod(b.shape) * b.dtype.itemsize for b in copied + buffers)
    good = (
        n in SCHEDULES
        and tp == 4
        and n & (n - 1) == 0
        and dims.heads == 8
        and wg.shape[0] == 1
        and ids.shape[1] == 2
        and experts <= LANES
        and dims.cap <= LANES
        and dims.cap % 16 == 0
        and held <= VMEM_BYTES
    )
    return dims if good else None


def on_device(
    tokens_a,
    attn_gain,
    w_query,
    w_query_rot,
    w_latent,
    w_key_rot,
    latent_gain,
    w_key_up,
    w_value_up,
    w_output,
    tokens_b,
    ffn_gain,
    expert_ids,
    expert_weights,
    w_gate,
    w_up,
    w_down,
):
    args = (
        tokens_a, attn_gain, w_query, w_query_rot, w_latent, w_key_rot, latent_gain, w_key_up,
        w_value_up, w_output, tokens_b, ffn_gain, expert_ids, expert_weights, w_gate, w_up, w_down,
    )
    dims = fused_dims(args)
    if dims is not None:
        return fused(dims, args)
    expert_count = w_gate.shape[0] * lax.axis_size("ep")
    outgoing, before = dispatch_rows(tokens_b, ffn_gain, expert_ids, expert_count)
    mixed_a, arrived = attention_half(
        tokens_a,
        attn_gain,
        w_query,
        w_query_rot,
        w_latent,
        w_key_rot,
        latent_gain,
        w_key_up,
        w_value_up,
        w_output,
        outgoing,
    )
    mixed_b = expert_half(arrived, before, expert_ids, expert_weights, w_gate, w_up, w_down)
    return (mixed_a, mixed_b)


def solution(mesh):
    placed = (
        P("ep", None),
        P(),
        P(None, "tp"),
        P(None, "tp"),
        P(),
        P(),
        P(),
        P(None, "tp"),
        P(None, "tp"),
        P("tp", None),
        P("ep", None),
        P(),
        P("ep", None),
        P("ep", None),
        P("ep", None, "tp"),
        P("ep", None, "tp"),
        P("ep", "tp", None),
    )
    return jax.shard_map(
        on_device,
        mesh=mesh,
        in_specs=placed,
        out_specs=(P(("ep", "tp"), None), P("ep", "tp")),
        check_vma=False,
    )
```

```python
import dataclasses
import functools
import math

import jax
import jax.numpy as jnp
import numpy as np
from jax import lax
from jax.experimental import pallas as pl
from jax.experimental.pallas import tpu as pltpu
from jax.sharding import PartitionSpec as P

NOPE = 64
ROPE = 32
VD = 64
LANES = 128
VMEM_BYTES = 60 * 1024 * 1024


epsilon = 1e-06
rope_base = 10000.0


def normalize(matrix, gain):
    floats = matrix.astype(jnp.float32)
    scaled = floats * lax.rsqrt(jnp.mean(floats * floats, axis=-1, keepdims=True) + epsilon)
    return scaled * gain


def rotate(vectors, positions):
    rot_width = vectors.shape[-1]
    half_width = rot_width // 2
    inverse = rope_base ** (-(jnp.arange(half_width, dtype=jnp.float32) * 2.0) / rot_width)
    angles = positions.astype(jnp.float32)[:, None] * inverse[None, :]
    cosine = jnp.cos(angles)[:, None, :]
    sine_part = jnp.sin(angles)[:, None, :]
    first_half = vectors[..., :half_width]
    second_half = vectors[..., half_width:]
    return jnp.concatenate(
        [
            first_half * cosine - second_half * sine_part,
            first_half * sine_part + second_half * cosine,
        ],
        axis=-1,
    )


def attention_half(
    tokens_a,
    attn_gain,
    w_query,
    w_query_rot,
    w_latent,
    w_key_rot,
    latent_gain,
    w_key_up,
    w_value_up,
    w_output,
    outgoing,
):
    row_count = tokens_a.shape[0]
    head_count = w_query.shape[1] // NOPE
    offset = lax.axis_index("ep") * row_count
    positions = offset + jnp.arange(row_count, dtype=jnp.int32)
    normed = normalize(tokens_a, attn_gain).astype(jnp.bfloat16)
    query_plain = jnp.dot(normed, w_query, preferred_element_type=jnp.float32).astype(jnp.bfloat16)
    query_plain = query_plain.reshape(row_count, head_count, NOPE)
    turned = jnp.dot(normed, w_query_rot, preferred_element_type=jnp.float32).reshape(
        row_count, head_count, ROPE
    )
    query_rotated_rows = rotate(turned, positions).astype(jnp.bfloat16)
    latent = normalize(
        jnp.dot(normed, w_latent, preferred_element_type=jnp.float32), latent_gain
    ).astype(jnp.bfloat16)
    key_raw = jnp.dot(normed, w_key_rot, preferred_element_type=jnp.float32)[:, None, :]
    key_turned = rotate(key_raw, positions)[:, 0, :].astype(jnp.bfloat16)
    logit_scale = (NOPE + ROPE) ** (-0.5)
    outgoing, compact = lax.optimization_barrier(
        (outgoing, jnp.concatenate([latent, key_turned], axis=1))
    )
    joined = lax.all_gather(compact, "ep", axis=0, tiled=True)
    arrived = lax.all_to_all(outgoing, "ep", split_axis=0, concat_axis=0, tiled=True)
    pieces = (joined[:, : latent.shape[1]], joined[:, latent.shape[1] :])
    piece_keys = jnp.dot(pieces[0], w_key_up, preferred_element_type=jnp.float32).astype(
        jnp.bfloat16
    )
    piece_values = jnp.dot(pieces[0], w_value_up, preferred_element_type=jnp.float32).astype(
        jnp.bfloat16
    )
    key_count = piece_keys.shape[0]
    blocks = key_count // row_count
    key_blocks = piece_keys.reshape(blocks, row_count, head_count, NOPE)
    value_blocks = piece_values.reshape(blocks, row_count, head_count, VD)
    rotated_key_blocks = pieces[1].reshape(blocks, row_count, ROPE)
    score_matrix = (
        jnp.einsum("yvz,wrvz->yvwr", query_plain, key_blocks, preferred_element_type=jnp.float32)
        + jnp.einsum(
            "yjx,inx->yjin",
            query_rotated_rows,
            rotated_key_blocks,
            preferred_element_type=jnp.float32,
        )
    ) * logit_scale
    key_pos = jnp.arange(key_count, dtype=jnp.int32).reshape(blocks, row_count)
    allowed = key_pos[None, None, :, :] <= positions[:, None, None, None]
    masked = jnp.where(allowed, score_matrix, -1e30)
    block_max = jnp.max(masked, axis=-1)
    probs = jnp.where(allowed, jnp.exp(masked - block_max[..., None]), 0.0)
    block_total = jnp.sum(probs, axis=-1)
    block_out = jnp.einsum(
        "qhbk,bkhd->qhbd",
        probs.astype(jnp.bfloat16),
        value_blocks,
        preferred_element_type=jnp.float32,
    )
    run_max = jnp.full((row_count, head_count), -1e30, jnp.float32)
    new_max = jnp.maximum(run_max, jnp.max(block_max, axis=-1))
    new_factor = jnp.exp(block_max - new_max[..., None])
    new_total = jnp.sum(new_factor * block_total, axis=-1)
    new_out = jnp.sum(new_factor[..., None] * block_out, axis=2)
    attended = (
        (new_out / new_total[..., None]).astype(jnp.bfloat16).reshape(row_count, head_count * VD)
    )
    mixed = lax.psum_scatter(
        jnp.dot(attended, w_output, preferred_element_type=jnp.float32).astype(jnp.bfloat16),
        "tp",
        scatter_dimension=0,
        tiled=True,
    )
    return mixed, arrived


def dispatch_rows(tokens_b, ffn_gain, expert_ids, expert_count):
    row_count, width = tokens_b.shape
    top_count = expert_ids.shape[1]
    capacity = 2 * row_count * top_count // expert_count
    tp_count = lax.axis_size("tp")
    part_width = width // tp_count
    floats = tokens_b.astype(jnp.float32)
    factor = lax.rsqrt(jnp.mean(floats * floats, axis=-1, keepdims=True) + epsilon)
    start = lax.axis_index("tp") * part_width
    own = lax.dynamic_slice_in_dim(tokens_b, start, part_width, 1).astype(jnp.float32)
    own_gain = lax.dynamic_slice_in_dim(ffn_gain, start, part_width, 0)
    normed = (own * factor * own_gain).astype(jnp.bfloat16)
    experts = jnp.arange(expert_count, dtype=jnp.int32)
    slots = jnp.arange(capacity, dtype=jnp.int32)
    named = (expert_ids[:, :, None] == experts).any(axis=1)
    rows = jnp.arange(row_count, dtype=jnp.int32)
    earlier = (rows[:, None] > rows[None, :]).astype(jnp.bfloat16)
    before = jnp.dot(
        earlier, named.astype(jnp.bfloat16), preferred_element_type=jnp.float32
    ).astype(jnp.int32)
    slot_of = jnp.where(named, before, -1).T
    chosen = (slot_of[:, None, :] == slots[None, :, None]).astype(jnp.bfloat16)
    outgoing = jnp.dot(
        chosen.reshape(expert_count * capacity, row_count),
        normed,
        preferred_element_type=jnp.float32,
    ).astype(jnp.bfloat16)
    outgoing = outgoing.reshape(expert_count, capacity, part_width)
    return outgoing, before


def swap(block, distance, count):
    return lax.ppermute(block, "tp", [(i, i ^ distance) for i in range(count)])


def expert_half(arrived, before, expert_ids, expert_weights, w_gate, w_up, w_down):
    expert_count, capacity, part_width = arrived.shape
    tp_count = lax.axis_size("tp")
    top_count = expert_ids.shape[1]
    experts = jnp.arange(expert_count, dtype=jnp.int32)
    me = lax.axis_index("tp")
    blocks = {0: arrived.reshape(-1, part_width)}
    distance = tp_count // 2
    while distance:
        for mask in list(blocks):
            blocks[mask ^ distance] = swap(blocks[mask], distance, tp_count)
        distance //= 2
    gate_part = 0.0
    up_part = 0.0
    for mask, block in blocks.items():
        first = (me ^ mask) * part_width
        gate_rows = lax.dynamic_slice_in_dim(w_gate[0], first, part_width, 0)
        up_rows = lax.dynamic_slice_in_dim(w_up[0], first, part_width, 0)
        gate_part += jnp.dot(block, gate_rows, preferred_element_type=jnp.float32)
        up_part += jnp.dot(block, up_rows, preferred_element_type=jnp.float32)
    hidden = (jax.nn.silu(gate_part) * up_part).astype(jnp.bfloat16)
    parts = {}
    for mask in reversed(range(tp_count)):
        down_columns = lax.dynamic_slice_in_dim(w_down[0], (me ^ mask) * part_width, part_width, 1)
        parts[mask] = jnp.dot(hidden, down_columns, preferred_element_type=jnp.float32)
    distance = 1
    while distance < tp_count:
        for mask in [m for m in parts if m & distance]:
            came = swap(parts.pop(mask).astype(jnp.bfloat16), distance, tp_count)
            parts[mask ^ distance] += came.astype(jnp.float32)
        distance *= 2
    summed = parts[0].astype(jnp.bfloat16)
    returned = lax.all_to_all(
        summed.reshape(expert_count, capacity, part_width),
        "ep",
        split_axis=0,
        concat_axis=0,
        tiled=True,
    )
    shares = expert_weights / jnp.sum(expert_weights, axis=1, keepdims=True)
    table = returned.reshape(expert_count * capacity, part_width)
    total = 0.0
    for k in range(top_count):
        own_slot = jnp.sum(jnp.where(expert_ids[:, k : k + 1] == experts, before, 0), axis=1)
        target = expert_ids[:, k] * capacity + own_slot
        pick = (
            target[:, None] == jnp.arange(expert_count * capacity, dtype=jnp.int32)
        ).astype(jnp.bfloat16)
        picked = jnp.dot(pick, table, preferred_element_type=jnp.float32)
        total = total + picked * shares[:, k : k + 1]
    return total.astype(jnp.bfloat16)


DOUBLED = (1, 2, 3)
UNMIXED = (0, 1, 2)


SCHEDULES = {
    8: (
        "D2", "enter", "S2", "D1", "S1", "D4", "S4", "own", "weights", "E0", "latents", "D5", "S5", "D6", "S6", "P0", "D3", "S3", "queries", "tables",
        "F2", "F1", "R1", "E1", "F4", "R2", "E2", "U1", "D7", "S7", "R4", "P1", "E4", "F5", "P2", "P4", "F6", "C0", "blank", "R5", "E5", "G4", "P5", "F7", "U2",
        "R6", "F3", "R3", "E6", "G5", "E3", "P6", "U3", "C1", "V0", "V1", "R7", "P3", "V2", "E7", "C2", "P7", "V3", "G6", "N",
        "W", "keys", "G3", "A0", "A1", "G7", "A2", "A3", "project", "C4", "C5", "pair", "C6", "C7", "C3", "M",
    )
}


def rope_tables(rows, blocks):
    half = ROPE // 2
    lane = np.arange(LANES) % ROPE
    inverse = rope_base ** (-((lane % half).astype(np.float64) * 2.0) / ROPE)
    near = np.arange(rows, dtype=np.float64)[:, None] * inverse[None, :]
    far = (np.arange(blocks, dtype=np.float64) * rows)[:, None] * inverse[None, :]
    pack = lambda v: np.asarray(v, np.float32)
    return pack(np.stack([np.cos(near), np.sin(near)])), pack(
        np.stack([np.cos(far), np.sin(far)], axis=1)
    )


def staged_as(step):
    @functools.wraps(step)
    def run(*given, **options):
        with jax.named_scope("_".join([step.__name__, *map(str, given)])):
            return step(*given, **options)

    return run


def fused_kernel(
    dims,
    ta_hbm, ag_hbm, wq_hbm, wqr_hbm, wl_hbm, wkr_hbm, lg_hbm, wku_hbm, wvu_hbm, wo_hbm,
    tb_hbm, fg_hbm, ids_hbm, wts_hbm, wg_hbm, wu_hbm, wd_hbm, near_hbm, far_hbm,
    out_a, out_b,
    ta, ag_ref, wq, wqr, wl, wkr, lg_ref, wku, wvu, wo,
    tb, fg_ref, ids_ref, wts_ref, wg, wu, wd, near_ref, far_ref,
    own_b, slot_t, slot_c, share_c, staged, wider, landed, part_keep, part_send, part_recv,
    pair_send, pair_recv, back_send, back_recv, side_send, side_recv, total, total_side, near_send, near_recv,
    normed_a, rot_w, lat, qs, keys, vals, att, mixed, am_send, am_recv, ax_send, ax_recv,
    load_sem, z_send, z_recv, x_send, x_recv, c_send, c_recv, f_send, f_recv,
    p_send, p_recv, q_send, q_recv, b_send, b_recv, s_send, s_recv, n_send, n_recv,
    lz_send, lz_recv, ly_send, ly_recv, ld_send, ld_recv, as_send, as_recv, at_send, at_recv,
):
    n, cap, rows_a, rows_b = dims.n, dims.cap, dims.rows_a, dims.rows_b
    width = dims.width
    e, t = lax.axis_index("ep"), lax.axis_index("tp")
    core = lax.rem(t, 2)
    mate, across = t + 1 - 2 * core, lax.rem(t + 2, 4)
    third = lax.rem(mate + 2, 4)
    quarter = (t, mate, across, third)
    floors, floor = n // 2, e // 2
    beside = e + 1 - 2 * lax.rem(e, 2)

    def partner(m):
        there, bit = e, 1
        while bit < n:
            if m & bit:
                there = there + bit - 2 * bit * lax.rem(e // bit, 2)
            bit *= 2
        return there

    def remote(src, dst, ssem, rsem, ep=None, tp=None):
        target = (e if ep is None else ep, t if tp is None else tp)
        return pltpu.make_async_remote_copy(
            src_ref=src, dst_ref=dst, send_sem=ssem, recv_sem=rsem,
            device_id=target, device_id_type=pl.DeviceIdType.MESH,
        )

    pairs = [
        (ids_hbm, ids_ref), (tb_hbm, tb), (fg_hbm, fg_ref), (ta_hbm, ta), (ag_hbm, ag_ref),
        (wl_hbm, wl), (wkr_hbm, wkr), (lg_hbm, lg_ref), (near_hbm, near_ref), (far_hbm, far_ref),
        (wg_hbm, wg), (wu_hbm, wu), (wd_hbm, wd), (wq_hbm, wq), (wqr_hbm, wqr),
        (wts_hbm, wts_ref), (wku_hbm, wku), (wvu_hbm, wvu), (wo_hbm, wo),
    ]
    loads = [pltpu.make_async_copy(s, d, load_sem.at[i]) for i, (s, d) in enumerate(pairs)]
    for load in loads:
        load.start()
    (l_ids, l_tb, l_fg, l_ta, l_ag, l_wl, l_wkr, l_lg, l_near, l_far) = loads[:10]
    (l_wg, l_wu, l_wd, l_wq, l_wqr, l_wts, l_wku, l_wvu, l_wo) = loads[10:]

    barrier = pltpu.get_barrier_semaphore()
    for k in range(1, n):
        pl.semaphore_signal(
            barrier, inc=1, device_id=(partner(k), t), device_id_type=pl.DeviceIdType.MESH
        )
    for peer in (mate, across):
        pl.semaphore_signal(
            barrier, inc=1, device_id=(e, peer), device_id_type=pl.DeviceIdType.MESH
        )

    def own_columns(which):
        return pl.ds(pl.multiple_of(which * width, width), width)

    with jax.named_scope("slots"):
        l_ids.wait()
        ids = ids_ref[...]
        sub = lax.broadcasted_iota(jnp.int32, (LANES, rows_b), 0)
        first, second = ids[0:1] == sub, ids[1:2] == sub
        named = jnp.logical_or(first, second)
        earlier = (
            lax.broadcasted_iota(jnp.int32, (rows_b, rows_b), 0)
            < lax.broadcasted_iota(jnp.int32, (rows_b, rows_b), 1)
        ).astype(jnp.float32).astype(jnp.bfloat16)
        before = jnp.dot(
            named.astype(jnp.float32).astype(jnp.bfloat16),
            earlier,
            preferred_element_type=jnp.float32,
        )
        slot = jnp.where(named, before, -1.0)
        slot_t[...] = slot

    with jax.named_scope("wait_tb"):
        l_tb.wait()
        l_fg.wait()
    with jax.named_scope("norm_b"):
        floats = tb[...].astype(jnp.float32)
        factor = lax.rsqrt(jnp.mean(floats * floats, axis=-1, keepdims=True) + epsilon)
        for mask in (0, 2):
            columns = own_columns(quarter[mask])
            own_b[mask] = (
                tb[:, columns].astype(jnp.float32) * factor * fg_ref[:, columns]
            ).astype(jnp.bfloat16)

    def z_copy(m):
        return remote(staged.at[m], landed.at[0, m], z_send.at[m], z_recv.at[m], ep=partner(m))

    def w_copy(m):
        return remote(
            wider.at[m], landed.at[2, m], x_send.at[m], x_recv.at[m], ep=partner(m)
        )

    def x_copy(m):
        return remote(landed.at[0, m], landed.at[2, m], x_send.at[m], x_recv.at[m], tp=across)

    def c_copy(m):
        return remote(landed.at[0, m], landed.at[1, m], c_send.at[m], c_recv.at[m], tp=mate)

    def f_copy(m):
        return remote(landed.at[2, m], landed.at[3, m], f_send.at[m], f_recv.at[m], tp=mate)

    def p_copy(m):
        return remote(part_send.at[m], part_recv.at[m], p_send.at[m], p_recv.at[m], tp=mate)

    def q_copy(m):
        return remote(pair_send.at[m], pair_recv.at[m], q_send.at[m], q_recv.at[m], tp=across)

    def b_copy(m):
        return remote(back_send.at[m], back_recv.at[m], b_send.at[m], b_recv.at[m], ep=partner(m))

    def s_copy(m):
        return remote(
            side_send.at[m], side_recv.at[m], s_send.at[m], s_recv.at[m], ep=partner(m)
        )

    def chosen_for(m):
        row = slot_t[pl.ds(partner(m), 1), :]
        wanted = lax.broadcasted_iota(jnp.int32, (cap, rows_b), 0).astype(jnp.float32)
        return (row == wanted).astype(jnp.float32).astype(jnp.bfloat16)

    @staged_as
    def dispatch(m):
        chosen = chosen_for(m)
        staged[m] = jnp.dot(chosen, own_b[0], preferred_element_type=jnp.float32).astype(
            jnp.bfloat16
        )
        if m in DOUBLED:
            wider[m] = jnp.dot(chosen, own_b[2], preferred_element_type=jnp.float32).astype(
                jnp.bfloat16
            )

    @staged_as
    def send(m):
        z_copy(m).start()
        if m in DOUBLED:
            w_copy(m).start()

    @staged_as
    def enter():
        pl.semaphore_wait(barrier, n + 1)

    @staged_as
    def keep_own():
        floats = tb[...].astype(jnp.float32)
        factor = lax.rsqrt(jnp.mean(floats * floats, axis=-1, keepdims=True) + epsilon)
        for mask in (1, 3):
            columns = own_columns(quarter[mask])
            own_b[mask] = (
                tb[:, columns].astype(jnp.float32) * factor * fg_ref[:, columns]
            ).astype(jnp.bfloat16)
        chosen = chosen_for(0)
        for mask in range(4):
            landed[mask, 0] = jnp.dot(
                chosen, own_b[mask], preferred_element_type=jnp.float32
            ).astype(jnp.bfloat16)

    @staged_as
    def tables():
        slot_c[...] = slot_t[...].T
        ids = ids_ref[...]
        sub = lax.broadcasted_iota(jnp.int32, (LANES, rows_b), 0)
        l_wts.wait()
        weight = wts_ref[...]
        sum_weight = weight[0:1] + weight[1:2]
        share_c[...] = (
            jnp.where(ids[0:1] == sub, weight[0:1] / sum_weight, 0.0)
            + jnp.where(ids[1:2] == sub, weight[1:2] / sum_weight, 0.0)
        ).T

    @staged_as
    def forward(m):
        with jax.named_scope(f"wait_z_copy_{m}"):
            z_copy(m).wait_recv()
        if m not in DOUBLED:
            x_copy(m).start()
        c_copy(m).start()

    @staged_as
    def relay(m):
        with jax.named_scope(f"wait_x_copy_{m}"):
            (w_copy if m in DOUBLED else x_copy)(m).wait_recv()
        f_copy(m).start()

    @staged_as
    def expert(m):
        if m:
            with jax.named_scope(f"wait_c_copy_{m}"):
                c_copy(m).wait_recv()
            with jax.named_scope(f"wait_f_copy_{m}"):
                f_copy(m).wait_recv()
        gate = up = None
        for mask in range(4):
            at = own_columns(quarter[mask])
            block = landed[mask, m]
            g = jnp.dot(block, wg[0, at, :], preferred_element_type=jnp.float32)
            u = jnp.dot(block, wu[0, at, :], preferred_element_type=jnp.float32)
            gate, up = (g, u) if mask == 0 else (gate + g, up + u)
        hidden = (gate / (1.0 + jnp.exp(-gate)) * up).astype(jnp.bfloat16)
        for place, mask in enumerate((1, 3)):
            part_send[m, place] = jnp.dot(
                hidden, wd[0, :, own_columns(quarter[mask])], preferred_element_type=jnp.float32
            ).astype(jnp.bfloat16)
        p_copy(m).start()
        for place, mask in enumerate((0, 2)):
            part_keep[m, place] = jnp.dot(
                hidden, wd[0, :, own_columns(quarter[mask])], preferred_element_type=jnp.float32
            )

    @staged_as
    def pair_sum(m):
        with jax.named_scope(f"wait_p_copy_{m}"):
            p_copy(m).wait_recv()
        side = (part_keep[m, 1] + part_recv[m, 1].astype(jnp.float32)).astype(jnp.bfloat16)
        if m in UNMIXED:
            own = (part_keep[m, 0] + part_recv[m, 0].astype(jnp.float32)).astype(jnp.bfloat16)
            if m:
                back_send[m] = own
                b_copy(m).start()
                side_send[m] = side
                s_copy(m).start()
            else:
                back_recv[0] = own
                side_recv[0] = side
            return
        pair_send[m] = side
        q_copy(m).start()
        part_keep[m, 0] = part_keep[m, 0] + part_recv[m, 0].astype(jnp.float32)

    @staged_as
    def give_back(m):
        with jax.named_scope(f"wait_q_copy_{m}"):
            q_copy(m).wait_recv()
        summed = (part_keep[m, 0] + pair_recv[m].astype(jnp.float32)).astype(jnp.bfloat16)
        if m:
            back_send[m] = summed
            b_copy(m).start()
        else:
            back_recv[0] = summed

    @staged_as
    def weights_in():
        l_wg.wait()
        l_wu.wait()
        l_wd.wait()

    @staged_as
    def combine(m):
        if m:
            with jax.named_scope(f"wait_b_copy_{m}"):
                b_copy(m).wait_recv()
        expert_at = partner(m)
        lane = lax.broadcasted_iota(jnp.int32, (rows_b, LANES), 1)
        here = lane == expert_at
        at = jnp.sum(jnp.where(here, slot_c[...], 0.0), axis=1, keepdims=True)
        share = jnp.sum(jnp.where(here, share_c[...], 0.0), axis=1, keepdims=True)
        wanted = lax.broadcasted_iota(jnp.int32, (rows_b, cap), 1).astype(jnp.float32)
        pick = (at == wanted).astype(jnp.float32).astype(jnp.bfloat16)
        picked = jnp.dot(pick, back_recv[m], preferred_element_type=jnp.float32) * share
        total[...] = total[...] + picked if m else picked
        if m in UNMIXED:
            if m:
                with jax.named_scope(f"wait_s_copy_{m}"):
                    s_copy(m).wait_recv()
            picked = jnp.dot(pick, side_recv[m], preferred_element_type=jnp.float32) * share
            total_side[...] = total_side[...] + picked if m else picked

    n_copy = remote(near_send, near_recv, n_send, n_recv, tp=across)

    @staged_as
    def near_out():
        near_send[...] = total_side[...].astype(jnp.bfloat16)
        n_copy.start()

    @staged_as
    def near_in():
        with jax.named_scope("wait_n_copy"):
            n_copy.wait_recv()
        total[...] = total[...] + near_recv[...].astype(jnp.float32)

    half_rows = rows_a // 2
    mine = pl.ds(pl.multiple_of(core * half_rows, half_rows), half_rows)
    yours = pl.ds(pl.multiple_of((1 - core) * half_rows, half_rows), half_rows)

    def under(k, other=False):
        return lax.rem((beside if other else e) + n - 2 * k, n)

    def passing(block, ssem, rsem, ep=None, tp=None):
        return remote(block, block, ssem, rsem, ep, tp)

    def lz_copy(k):
        return passing(
            lat.at[under(k), mine], lz_send.at[k], lz_recv.at[k + 1], ep=lax.rem(e + 2, n)
        )

    def lz_far():
        return passing(
            lat.at[under(1), mine], lz_send.at[2], lz_recv.at[3], ep=lax.rem(e + 4, n)
        )

    def lz_arrival(k):
        return passing(
            lat.at[under(k), mine], lz_send.at[k], lz_recv.at[k], ep=lax.rem(e + 2, n)
        )

    def ly_copy(k):
        return passing(lat.at[under(k), mine], ly_send.at[k], ly_recv.at[k], ep=beside)

    def ly_arrival(k):
        return passing(lat.at[under(k, True), mine], ly_send.at[k], ly_recv.at[k], ep=beside)

    def ld_copy(k, other, rows=None):
        j = k + floors * other
        block = lat.at[under(k, other), mine if rows is None else rows]
        return passing(block, ld_send.at[j], ld_recv.at[j], tp=mate)

    rising = floor < floors - 1
    rising_far = floor < floors - 2

    @staged_as
    def latents():
        l_ta.wait()
        l_ag.wait()
        rows = ta[...].astype(jnp.float32)
        scale = lax.rsqrt(jnp.mean(rows * rows, axis=-1, keepdims=True) + epsilon)
        normed_a[...] = (rows * scale * ag_ref[...]).astype(jnp.bfloat16)
        l_wl.wait()
        l_lg.wait()
        raw = jnp.dot(normed_a[...], wl[...], preferred_element_type=jnp.float32)
        scale = lax.rsqrt(jnp.mean(raw * raw, axis=-1, keepdims=True) + epsilon)
        lat[e, :, : dims.rank] = (raw * scale * lg_ref[...]).astype(jnp.bfloat16)
        l_wkr.wait()
        l_near.wait()
        l_far.wait()
        plain = wkr[...]
        swapped = jnp.concatenate([-plain[ROPE // 2 :], plain[: ROPE // 2]], axis=0)
        for copy in range(LANES // ROPE):
            rot_w[copy * ROPE : (copy + 1) * ROPE] = plain
            rot_w[LANES + copy * ROPE : LANES + (copy + 1) * ROPE] = swapped
        both = lax.dot_general(
            normed_a[...], rot_w[...], (((1,), (1,)), ((), ())), preferred_element_type=jnp.float32
        )
        cosine, sine = turn()
        lat[e, :, dims.rank :] = (both[:, :LANES] * cosine + both[:, LANES:] * sine).astype(
            jnp.bfloat16
        )
        pl.when(rising)(lz_copy(0).start)
        ly_copy(0).start()

    @staged_as
    def blank():
        for k in range(1, floors):

            @pl.when(floor + k < floors)
            def _():
                for side in range(2):
                    lat[2 * lax.rem(floor + k, floors) + side] = jnp.zeros(
                        lat.shape[1:], lat.dtype
                    )

    def turn():
        far = far_ref[e]
        cosine = near_ref[0] * far[0:1] - near_ref[1] * far[1:2]
        sine = near_ref[1] * far[0:1] + near_ref[0] * far[1:2]
        return cosine, sine

    @staged_as
    def latents_on(k):
        @pl.when(floor >= k)
        def _():
            with jax.named_scope("wait_lz"):
                lz_arrival(k).wait_recv()
            if k == 1:
                pl.when(rising)(lz_copy(1).start)
                pl.when(rising_far)(lz_far().start)
            ly_copy(k).start()
            ld_copy(k, False).start()

    @staged_as
    def latents_over(k):
        @pl.when(floor >= k)
        def _():
            with jax.named_scope("wait_ly"):
                ly_arrival(k).wait_recv()
            ld_copy(k, True).start()

    @staged_as
    def latents_in():
        for k in range(floors):

            @pl.when(floor >= k)
            def _():
                with jax.named_scope("wait_ld"):
                    if k:
                        ld_copy(k, False, yours).wait_recv()
                    ld_copy(k, True, yours).wait_recv()

    @staged_as
    def queries():
        l_wq.wait()
        l_wqr.wait()
        plain = jnp.dot(normed_a[...], wq[...], preferred_element_type=jnp.float32).astype(
            jnp.bfloat16
        )
        raw = jnp.dot(normed_a[...], wqr[...], preferred_element_type=jnp.float32)
        cosine, sine = turn()
        lane = lax.broadcasted_iota(jnp.int32, (rows_a, LANES), 1)
        low = lax.rem(lane, ROPE) < ROPE // 2
        turned = []
        for g in range(raw.shape[1] // LANES):
            x = raw[:, g * LANES : (g + 1) * LANES]
            other = jnp.where(
                low, -pltpu.roll(x, LANES - ROPE // 2, 1), pltpu.roll(x, ROPE // 2, 1)
            )
            turned.append(x * cosine + other * sine)
        for p in range(dims.heads // 2):
            wide = plain[:, p * LANES : (p + 1) * LANES].astype(jnp.float32)
            rot = turned[2 * p * ROPE // LANES]
            for side in range(2):
                at = (2 * p + side) * ROPE % LANES
                mine_wide = (lane // NOPE) == side
                mine_rot = (lane // ROPE) == at // ROPE
                own = slice(side * rows_a, (side + 1) * rows_a)
                qs[p, own, :LANES] = jnp.where(mine_wide, wide, 0.0).astype(jnp.bfloat16)
                qs[p, own, LANES:] = jnp.where(mine_rot, rot, 0.0).astype(jnp.bfloat16)

    @staged_as
    def key_values():
        l_wku.wait()
        l_wvu.wait()
        for j in range(n):
            keys[pl.ds(j * rows_a, rows_a), :] = jnp.dot(
                lat[j, :, : dims.rank], wku[...], preferred_element_type=jnp.float32
            ).astype(jnp.bfloat16)
            vals[pl.ds(j * rows_a, rows_a), :] = jnp.dot(
                lat[j, :, : dims.rank], wvu[...], preferred_element_type=jnp.float32
            ).astype(jnp.bfloat16)

    logit_scale = (NOPE + ROPE) ** (-0.5)

    @staged_as
    def attend(p):
        at = slice(p * LANES, (p + 1) * LANES)
        contract = (((1,), (1,)), ((), ()))
        scores = []
        for j in range(n):
            block = jnp.concatenate(
                [keys[j * rows_a : (j + 1) * rows_a, at], lat[j, :, dims.rank :]], axis=1
            )
            scores.append(
                lax.dot_general(qs[p], block, contract, preferred_element_type=jnp.float32)
            )
        score = jnp.concatenate(scores, axis=1) * logit_scale
        shape = score.shape
        position = e * rows_a + lax.rem(lax.broadcasted_iota(jnp.int32, shape, 0), rows_a)
        allowed = lax.broadcasted_iota(jnp.int32, shape, 1) <= position
        masked = jnp.where(allowed, score, -1e30)
        top = jnp.max(masked, axis=1, keepdims=True)
        probs = jnp.where(allowed, jnp.exp(masked - top), 0.0)
        weight_sum = jnp.sum(probs, axis=1, keepdims=True)
        got = jnp.dot(probs.astype(jnp.bfloat16), vals[:, at], preferred_element_type=jnp.float32)
        got = got / weight_sum
        lane = lax.broadcasted_iota(jnp.int32, (rows_a, LANES), 1)
        att[:, at] = jnp.where(lane < VD, got[:rows_a], got[rows_a:]).astype(jnp.bfloat16)

    share_rows = rows_a // 4

    def rows_of(which):
        return pl.ds(pl.multiple_of(which * share_rows, share_rows), share_rows)

    am_copy = remote(am_send, am_recv, as_send, as_recv, tp=mate)
    ax_copy = remote(ax_send, ax_recv, at_send, at_recv, tp=across)

    @staged_as
    def project():
        l_wo.wait()
        mixed[...] = jnp.dot(att[...], wo[...], preferred_element_type=jnp.float32).astype(
            jnp.bfloat16
        ).astype(jnp.float32)
        for place, mask in enumerate((1, 3)):
            am_send[place] = mixed[rows_of(quarter[mask]), :].astype(jnp.bfloat16)
        am_copy.start()

    @staged_as
    def project_pair():
        with jax.named_scope(f"wait_am_copy"):
            am_copy.wait_recv()
        ax_send[...] = (mixed[rows_of(across), :] + am_recv[1].astype(jnp.float32)).astype(
            jnp.bfloat16
        )
        ax_copy.start()

    @staged_as
    def project_end():
        with jax.named_scope(f"wait_ax_copy"):
            ax_copy.wait_recv()
        out_a[...] = (
            mixed[rows_of(t), :]
            + am_recv[0].astype(jnp.float32)
            + ax_recv[...].astype(jnp.float32)
        ).astype(jnp.bfloat16)

    stages = dict(
        D=dispatch, S=send, enter=enter, F=forward, R=relay, E=expert, P=pair_sum, G=give_back, C=combine,
        latents=latents, own=keep_own, queries=queries, tables=tables, blank=blank,
        U=latents_on, V=latents_over, W=latents_in, keys=key_values, A=attend,
        N=near_out, M=near_in, project=project, pair=project_pair, weights=weights_in,
    )
    for entry in SCHEDULES[n]:
        if entry in stages:
            stages[entry]()
        else:
            stages[entry[0]](int(entry[1:]))
    out_b[...] = total[...].astype(jnp.bfloat16)
    project_end()

    for m in range(1, n):
        for make in (z_copy, c_copy, f_copy, b_copy, w_copy if m in DOUBLED else x_copy):
            make(m).wait_send()
    for m in range(n):
        p_copy(m).wait_send()
        if m not in UNMIXED:
            q_copy(m).wait_send()
        elif m:
            s_copy(m).wait_send()
    n_copy.wait_send()
    for k in range(floors):

        @pl.when(floor >= k)
        def _():
            if k <= 1:
                pl.when(rising)(lz_copy(k).wait_send)
            if k == 1:
                pl.when(rising_far)(lz_far().wait_send)
            ly_copy(k).wait_send()
            if k:
                ld_copy(k, False).wait_send()
            ld_copy(k, True).wait_send()

    am_copy.wait_send()
    ax_copy.wait_send()


@dataclasses.dataclass(frozen=True)
class Dims:
    n: int
    cap: int
    rows_a: int
    rows_b: int
    width: int
    rank: int
    heads: int


def fused_scratch(dims, args):
    ta, wku, wvu = args[0], args[7], args[8]
    n, cap, width, rows_a, rows_b = dims.n, dims.cap, dims.width, dims.rows_a, dims.rows_b
    model = ta.shape[1]
    bf, f32 = jnp.bfloat16, jnp.float32
    vmem = pltpu.VMEM
    copied = [vmem(a.shape, a.dtype) for a in args]
    block = (cap, width)
    quarter_rows = rows_a // 4
    return copied, [
        vmem((4, rows_b, width), bf),
        vmem((LANES, rows_b), f32),
        vmem((rows_b, LANES), f32),
        vmem((rows_b, LANES), f32),
        vmem((n, *block), bf),
        vmem((n, *block), bf),
        vmem((4, n, *block), bf),
        vmem((n, 2, *block), f32),
        vmem((n, 2, *block), bf),
        vmem((n, 2, *block), bf),
        vmem((n, *block), bf),
        vmem((n, *block), bf),
        vmem((n, *block), bf),
        vmem((n, *block), bf),
        vmem((n // 2, *block), bf),
        vmem((n // 2, *block), bf),
        vmem((rows_b, width), f32),
        vmem((rows_b, width), f32),
        vmem((rows_b, width), bf),
        vmem((rows_b, width), bf),
        vmem((rows_a, model), bf),
        vmem((2 * LANES, model), bf),
        vmem((n, rows_a, dims.rank + LANES), bf),
        vmem((dims.heads // 2, 2 * rows_a, 2 * LANES), bf),
        vmem((n * rows_a, wku.shape[1]), bf),
        vmem((n * rows_a, wvu.shape[1]), bf),
        vmem((rows_a, wvu.shape[1]), bf),
        vmem((rows_a, model), f32),
        vmem((2, quarter_rows, model), bf),
        vmem((2, quarter_rows, model), bf),
        vmem((quarter_rows, model), bf),
        vmem((quarter_rows, model), bf),
    ]


def fused(dims, args):
    ta = args[0]
    args = fused_operands(dims, args)
    copied, buffers = fused_scratch(dims, args)
    n = dims.n
    dma = pltpu.SemaphoreType.DMA
    sems = [dma((len(copied),))] + [dma((n,)) for _ in range(16)] + [dma, dma]
    sems += [dma((n + 1,)) for _ in range(6)] + [dma, dma, dma, dma]
    inside = pl.BlockSpec(memory_space=pltpu.VMEM)
    return pl.pallas_call(
        functools.partial(fused_kernel, dims),
        out_shape=(
            pltpu.VMEM((dims.rows_a // 4, ta.shape[1]), jnp.bfloat16),
            pltpu.VMEM((dims.rows_b, dims.width), jnp.bfloat16),
        ),
        in_specs=[pl.BlockSpec(memory_space=pltpu.HBM)] * len(args),
        out_specs=(inside, inside),
        scratch_shapes=copied + buffers + sems,
        compiler_params=pltpu.CompilerParams(
            collective_id=0, has_side_effects=True, vmem_limit_bytes=VMEM_BYTES
        ),
        name="fused",
    )(*args)


def fused_operands(dims, args):
    (ta, ag, wq, wqr, wl, wkr, lg, wku, wvu, wo, tb, fg, ids, wts, wg, wu, wd) = args
    near, far = rope_tables(dims.rows_a, dims.n)
    return (
        ta, ag[None], wq, wqr, wl, wkr.T, lg[None], wku, wvu, wo, tb, fg[None], ids.T, wts.T,
        wg, wu, wd, jnp.asarray(near), jnp.asarray(far),
    )


def fused_dims(args):
    (ta, _, wq, wqr, wl, wkr, _, wku, wvu, wo, tb, _, ids, _, wg, _, wd) = args
    n, tp = lax.axis_size("ep"), lax.axis_size("tp")
    experts = wg.shape[0] * n
    dims = Dims(
        n=n,
        cap=2 * tb.shape[0] * ids.shape[1] // experts,
        rows_a=ta.shape[0],
        rows_b=tb.shape[0],
        width=tb.shape[1] // tp,
        rank=wl.shape[1],
        heads=wq.shape[1] // NOPE,
    )
    copied, buffers = fused_scratch(dims, args)
    held = sum(math.prod(b.shape) * b.dtype.itemsize for b in copied + buffers)
    good = (
        n in SCHEDULES
        and tp == 4
        and n & (n - 1) == 0
        and dims.heads == 8
        and wg.shape[0] == 1
        and ids.shape[1] == 2
        and experts <= LANES
        and dims.cap <= LANES
        and dims.cap % 16 == 0
        and held <= VMEM_BYTES
    )
    return dims if good else None


def on_device(
    tokens_a,
    attn_gain,
    w_query,
    w_query_rot,
    w_latent,
    w_key_rot,
    latent_gain,
    w_key_up,
    w_value_up,
    w_output,
    tokens_b,
    ffn_gain,
    expert_ids,
    expert_weights,
    w_gate,
    w_up,
    w_down,
):
    args = (
        tokens_a, attn_gain, w_query, w_query_rot, w_latent, w_key_rot, latent_gain, w_key_up,
        w_value_up, w_output, tokens_b, ffn_gain, expert_ids, expert_weights, w_gate, w_up, w_down,
    )
    dims = fused_dims(args)
    if dims is not None:
        return fused(dims, args)
    expert_count = w_gate.shape[0] * lax.axis_size("ep")
    outgoing, before = dispatch_rows(tokens_b, ffn_gain, expert_ids, expert_count)
    mixed_a, arrived = attention_half(
        tokens_a,
        attn_gain,
        w_query,
        w_query_rot,
        w_latent,
        w_key_rot,
        latent_gain,
        w_key_up,
        w_value_up,
        w_output,
        outgoing,
    )
    mixed_b = expert_half(arrived, before, expert_ids, expert_weights, w_gate, w_up, w_down)
    return (mixed_a, mixed_b)


def solution(mesh):
    placed = (
        P("ep", None),
        P(),
        P(None, "tp"),
        P(None, "tp"),
        P(),
        P(),
        P(),
        P(None, "tp"),
        P(None, "tp"),
        P("tp", None),
        P("ep", None),
        P(),
        P("ep", None),
        P("ep", None),
        P("ep", None, "tp"),
        P("ep", None, "tp"),
        P("ep", "tp", None),
    )
    return jax.shard_map(
        on_device,
        mesh=mesh,
        in_specs=placed,
        out_specs=(P(("ep", "tp"), None), P("ep", "tp")),
        check_vma=False,
    )
```
